128 devices in a mesh: sp: 32 (over z, y, core), tp: 4 (over x).
Axes of the slice: x: 4, y: 4, z: 4, core: 2. Of those that a mesh axis runs over, the one named last changes fastest.
Arguments:
- tokens: bfloat16 [8192, 2048], P('sp'), may hold values from -6 to 6
- input_norm_gain: float32 [2048], replicated, may hold values from 0.1 to 1.9
- convolution_value_weight: bfloat16 [2048, 512], P(None, 'tp'), may hold values from -0.125 to 0.125
- convolution_gate_weight: bfloat16 [2048, 512], P(None, 'tp'), may hold values from -0.125 to 0.125
- depthwise_taps_weight: float32 [31, 512], P(None, 'tp'), may hold values from -1 to 1
- convolution_group_gain: float32 [512], P('tp'), may hold values from 0.1 to 1.9
- convolution_group_shift: float32 [512], P('tp'), may hold values from -3 to 3
- receptance_weight: bfloat16 [2048, 1024], P(None, 'tp'), may hold values from -0.125 to 0.125
- key_weight: bfloat16 [2048, 1024], P(None, 'tp'), may hold values from -0.125 to 0.125
- value_weight: bfloat16 [2048, 1024], P(None, 'tp'), may hold values from -0.125 to 0.125
- decay_weight: bfloat16 [2048, 1024], P(None, 'tp'), may hold values from -0.0625 to 0.0625
- correction_rate_weight: bfloat16 [2048, 1024], P(None, 'tp'), may hold values from -0.125 to 0.125
- output_gate_weight: bfloat16 [2048, 1024], P(None, 'tp'), may hold values from -0.125 to 0.125
- key_prenorm_gain: float32 [1024], P('tp'), may hold values from 0.04 to 8
- decay_offset_bias: float32 [1024], P('tp'), may hold values from -30 to 0
- position_decay_shift: float32 [8192, 1024], P('sp', 'tp'), may hold values from -1 to 1
- extra_log_decay: float32 [8192, 1024], P('sp', 'tp'), may hold values from -0.7 to 0
- head_norm_gain: float32 [1024], P('tp'), may hold values from 0.1 to 1.9
- convolution_output_weight: bfloat16 [512, 2048], replicated, may hold values from -0.15625 to 0.15625
- attention_output_weight: bfloat16 [1024, 2048], replicated, may hold values from -0.15625 to 0.15625
Outputs:
- mixed: bfloat16 [8192, 2048], P(('sp', 'tp'))
The draws below stay inside these ranges and needn't reach their ends.
All inputs are finite; a program needn't handle non-finite values.
Results may differ from the reference program's by a relative error of at most 0.0063.
The reference program's roundings to bfloat16 on the way (of `normed`, `conv_input`, `conv_out` and `mix_out`) count: a program that leaves them out, or rounds other values in their place, can miss the bound.
Values may be sent and summed in bfloat16 or wider, within the bound.
A program may use at most 128 MiB of HBM per device.

```python
import jax
import jax.numpy as jnp
from jax import lax

D = 2048
CONV_CH = 512
CONV_TAPS = 31
HEADS = 16
HEAD = 64
TOKENS = 8192
MIX_CH = 1024


def draw_key_prenorm_gain(key, part):
    second = jax.random.fold_in(jax.random.fold_in(key, 53), 1)
    gain = jnp.exp(jnp.log(0.04) + jnp.log(200.0) * jax.random.uniform(second, (HEADS * HEAD,)))
    return jnp.clip(gain, 0.04, 8.0).astype(jnp.float32)


def draw_decay_offset_bias(key, part):
    first, second, third, fourth = jax.random.split(jax.random.fold_in(key, 11), 4)
    share = 0.5
    slow_head = jax.random.uniform(first, (HEADS,)) < share
    keep_scale = jnp.exp(jnp.log(0.1) + jnp.log(6.0) * jax.random.uniform(second, (HEADS,)))
    fast_length = jax.random.uniform(third, (HEADS,), minval=25.0, maxval=50.0)
    level = jnp.where(slow_head, jnp.log(keep_scale / TOKENS), -jnp.log(fast_length)) + 0.5
    jitter = jnp.clip(0.3 * jax.random.normal(fourth, (HEADS, HEAD)), -1.0, 1.0)
    return (level[:, None] + jitter).reshape(HEADS * HEAD).astype(jnp.float32)


def draw_position_decay_shift(key, part):
    level_key = jax.random.fold_in(key, 23)
    block_count = (TOKENS + 127) // 128
    level = jax.random.uniform(level_key, (block_count, HEADS), minval=-0.7, maxval=0.7)
    spread_rows = jnp.repeat(level, 128, axis=0)[:TOKENS]
    return jnp.repeat(spread_rows, HEAD, axis=1).astype(jnp.float32)


def draw_extra_log_decay(key, part):
    first, second = jax.random.split(jax.random.fold_in(key, 37), 2)
    places = jax.random.randint(first, (6,), 0, TOKENS)
    kept = jax.random.uniform(second, (6, HEADS * HEAD), minval=0.5, maxval=0.8)
    return jnp.zeros((TOKENS, HEADS * HEAD), jnp.float32).at[places].min(jnp.log(kept))


def level_of(stream_key, dims, pieces, smallest, top_value):
    def one(dim, shards_of):
        draws = jax.random.uniform(jax.random.fold_in(jax.random.fold_in(stream_key, 6), dim), (shards_of,), jnp.float32, smallest / len(pieces), top_value / len(pieces))
        return jnp.repeat(jnp.exp(draws), dims[dim] // shards_of).reshape((-1,) + (1,) * (len(dims) - dim - 1))

    factor_of = one(*pieces[0])
    for cut in pieces[1:]:
        factor_of = factor_of * one(*cut)
    return factor_of


def normal_values(rng, extent, spread, limit, cuts=(), kind=jnp.bfloat16):
    entries = spread * jax.random.normal(rng, extent, jnp.float32)
    if cuts:
        entries = entries * level_of(rng, extent, cuts, -0.22, 0.18)
    return jnp.clip(entries, -limit, limit).astype(kind)


def setup_inputs(seed: int = 0) -> dict:
    splits = jax.random.split(jax.random.key(seed), 21)
    tokens = normal_values(splits[0], (TOKENS, D), 1.0, 6.0, ((0, 32),))
    input_norm_gain = jnp.clip(1.0 + 0.18 * jax.random.normal(splits[1], (D,), jnp.float32), 0.1, 1.9)
    convolution_value_weight = normal_values(splits[2], (D, CONV_CH), D ** -0.5, 0.125, ((1, 4),))
    convolution_gate_weight = normal_values(splits[3], (D, CONV_CH), D ** -0.5, 0.125, ((1, 4),))
    depthwise_taps_weight = normal_values(splits[4], (CONV_TAPS, CONV_CH), CONV_TAPS ** -0.5, 1.0, ((1, 4),), jnp.float32)
    convolution_group_gain = jnp.clip(1.0 + 0.18 * jax.random.normal(splits[5], (CONV_CH,), jnp.float32), 0.1, 1.9)
    convolution_group_shift = normal_values(splits[6], (CONV_CH,), 0.5, 3.0, ((0, 4),), jnp.float32)
    receptance_weight = normal_values(splits[7], (D, MIX_CH), D ** -0.5, 0.125, ((1, 4),))
    key_weight = normal_values(splits[8], (D, MIX_CH), D ** -0.5, 0.125, ((1, 4),))
    value_weight = normal_values(splits[9], (D, MIX_CH), D ** -0.5, 0.125, ((1, 4),))
    decay_weight = normal_values(splits[10], (D, MIX_CH), (4 * D) ** -0.5, 0.0625, ((1, 4),))
    correction_rate_weight = normal_values(splits[11], (D, MIX_CH), D ** -0.5, 0.125, ((1, 4),))
    output_gate_weight = normal_values(splits[12], (D, MIX_CH), D ** -0.5, 0.125, ((1, 4),))
    key_prenorm_gain = draw_key_prenorm_gain(jax.random.fold_in(splits[20], 71), 0)
    decay_offset_bias = draw_decay_offset_bias(jax.random.fold_in(splits[20], 71), 0)
    position_decay_shift = draw_position_decay_shift(jax.random.fold_in(splits[20], 71), 0)
    extra_log_decay = draw_extra_log_decay(jax.random.fold_in(splits[20], 71), 0)
    head_norm_gain = jnp.clip(1.0 + 0.18 * jax.random.normal(splits[17], (MIX_CH,), jnp.float32), 0.1, 1.9)
    convolution_output_weight = normal_values(splits[18], (CONV_CH, D), (CONV_CH + MIX_CH) ** -0.5, 0.15625)
    attention_output_weight = normal_values(splits[19], (MIX_CH, D), (CONV_CH + MIX_CH) ** -0.5, 0.15625)
    return dict(tokens=tokens, input_norm_gain=input_norm_gain, convolution_value_weight=convolution_value_weight, convolution_gate_weight=convolution_gate_weight, depthwise_taps_weight=depthwise_taps_weight, convolution_group_gain=convolution_group_gain, convolution_group_shift=convolution_group_shift, receptance_weight=receptance_weight, key_weight=key_weight, value_weight=value_weight, decay_weight=decay_weight, correction_rate_weight=correction_rate_weight, output_gate_weight=output_gate_weight, key_prenorm_gain=key_prenorm_gain, decay_offset_bias=decay_offset_bias, position_decay_shift=position_decay_shift, extra_log_decay=extra_log_decay, head_norm_gain=head_norm_gain, convolution_output_weight=convolution_output_weight, attention_output_weight=attention_output_weight)


NORM_EPS = 1e-06
GROUP_EPS = 1e-05
HEAD_EPS = 0.00064
KEY_EPS = 1e-06

def stored(values):
    return lax.optimization_barrier(values.astype(jnp.bfloat16)).astype(jnp.float32)

def recurrence_step(state, inputs):
    receptance, decay, key_row, value_row, unit_key, erase_dir = inputs
    removed = jnp.einsum('hij,hj->hi', state, -unit_key)
    state = state * decay[:, None, :] + removed[:, :, None] * erase_dir[:, None, :] + value_row[:, :, None] * key_row[:, None, :]
    return (state, jnp.einsum('hij,hj->hi', state, receptance))

def reference(tokens, input_norm_gain, convolution_value_weight, convolution_gate_weight, depthwise_taps_weight, convolution_group_gain, convolution_group_shift, receptance_weight, key_weight, value_weight, decay_weight, correction_rate_weight, output_gate_weight, key_prenorm_gain, decay_offset_bias, position_decay_shift, extra_log_decay, head_norm_gain, convolution_output_weight, attention_output_weight):
    float_rows = tokens.astype(jnp.float32)
    normed = (float_rows * lax.rsqrt(lax.optimization_barrier(jnp.mean(float_rows * float_rows, axis=-1, keepdims=True)) + NORM_EPS) * input_norm_gain).astype(jnp.bfloat16)

    def project(weight):
        return stored(jnp.dot(normed, weight, preferred_element_type=jnp.float32))
    conv_input = stored(project(convolution_value_weight) * jax.nn.sigmoid(project(convolution_gate_weight)))
    padded = jnp.pad(conv_input, ((CONV_TAPS - 1, 0), (0, 0)))
    conv_sum = jnp.zeros((TOKENS, CONV_CH), jnp.float32)
    for offset in range(CONV_TAPS):
        conv_sum = conv_sum + depthwise_taps_weight[offset] * padded[offset:offset + TOKENS]
    grouped = conv_sum.reshape(TOKENS, CONV_CH // 64, 64)
    centred = grouped - lax.optimization_barrier(jnp.mean(grouped, axis=-1, keepdims=True))
    grouped = centred * lax.rsqrt(lax.optimization_barrier(jnp.mean(centred * centred, axis=-1, keepdims=True)) + GROUP_EPS)
    conv_out = jax.nn.silu(grouped.reshape(TOKENS, CONV_CH) * convolution_group_gain + convolution_group_shift).astype(jnp.bfloat16)
    receptance = project(receptance_weight)
    key_all = project(key_weight)
    value_all = project(value_weight)
    decay_logits = project(decay_weight) + decay_offset_bias + position_decay_shift
    decay_logarithm = -jnp.exp(-jax.nn.softplus(-decay_logits) - 0.5) + extra_log_decay
    erase_rate = jax.nn.sigmoid(project(correction_rate_weight))
    out_gate = jax.nn.sigmoid(project(output_gate_weight))

    def by_head(values):
        return values.reshape(TOKENS, HEADS, HEAD)
    unit_key = by_head(key_all * key_prenorm_gain)
    unit_key = unit_key * lax.rsqrt(lax.optimization_barrier(jnp.sum(unit_key * unit_key, axis=-1, keepdims=True)) + KEY_EPS)
    erase_dir = unit_key * by_head(erase_rate)
    start_state = jnp.zeros((HEADS, HEAD, HEAD), jnp.float32)
    _, readout = lax.scan(recurrence_step, start_state, (by_head(receptance), by_head(jnp.exp(decay_logarithm)), by_head(key_all), by_head(value_all), unit_key, erase_dir))
    centred_read = readout - lax.optimization_barrier(jnp.mean(readout, axis=-1, keepdims=True))
    normed_read = centred_read * lax.rsqrt(lax.optimization_barrier(jnp.mean(centred_read * centred_read, axis=-1, keepdims=True)) + HEAD_EPS)
    mix_out = (normed_read.reshape(TOKENS, HEADS * HEAD) * head_norm_gain * out_gate).astype(jnp.bfloat16)
    projected = jnp.dot(conv_out, convolution_output_weight, preferred_element_type=jnp.float32) + jnp.dot(mix_out, attention_output_weight, preferred_element_type=jnp.float32)
    return projected.astype(jnp.bfloat16)
```

```python
import functools

import jax
import jax.numpy as jnp
from jax import lax
from jax.experimental import pallas as pl
from jax.experimental.pallas import tpu as pltpu
from jax.sharding import PartitionSpec as P

F32 = jnp.float32
BF16 = jnp.bfloat16
MESH = pl.DeviceIdType.MESH
HEAD = 64
CHUNK = 64
PAIR = 128

NORM_EPS = 1e-06
GROUP_EPS = 1e-05
HEAD_EPS = 0.00064
KEY_EPS = 1e-06

NN = (((1,), (0,)), ((), ()))
NT = (((1,), (1,)), ((), ()))


def dot(left, right, dims=NN):
    return lax.dot_general(left, right, dims, preferred_element_type=F32)


def split(values):
    high = values.astype(BF16)
    return high, (values - high.astype(F32)).astype(BF16)


def dot1(left, right, dims=NN):
    return dot(left.astype(BF16), right.astype(BF16), dims)


def dot3(left, right, dims=NN):
    left_high, left_low = split(left)
    right_high, right_low = split(right)
    return dot(left_high, right_high, dims) + (
        dot(left_low, right_high, dims) + dot(left_high, right_low, dims)
    )


def dot2(left, right_exact):
    high, low = split(left)
    return dot(high, right_exact) + dot(low, right_exact)


def iota(shape, dim):
    return lax.broadcasted_iota(jnp.int32, shape, dim)


def first_head(rows):
    return iota((rows, PAIR), 1) < HEAD


def diagonal(packed):
    mask = first_head(packed.shape[0])
    return jnp.concatenate([jnp.where(mask, packed, 0.0), jnp.where(mask, 0.0, packed)], axis=0)


def undiagonal(full):
    return jnp.where(first_head(HEAD), full[:HEAD], full[HEAD:])


def beside(*parts):
    return jnp.concatenate(parts, axis=1)


def group_ones(width):
    return (iota((width, width), 0) // HEAD == iota((width, width), 1) // HEAD).astype(BF16)


def sigmoid(values):
    return 1.0 / (1.0 + jnp.exp(-values))


def rounded(values):
    return values.astype(BF16).astype(F32)


def normalize(tokens, gain):
    rows = tokens.astype(F32)
    scale = lax.rsqrt(jnp.mean(rows * rows, axis=-1, keepdims=True) + NORM_EPS)
    return (rows * scale * gain).astype(BF16)


def group_norm(values, ones, eps):
    centred = values - dot2(values, ones) * (1.0 / HEAD)
    return centred * lax.rsqrt(dot2(centred * centred, ones) * (1.0 / HEAD) + eps)


def compose(later, earlier, product):
    trans, base = later
    out = product(trans, beside(diagonal(earlier[0]), diagonal(earlier[1])))
    return out[:, :PAIR], out[:, PAIR:] + base


def chunk_algebra(receptance, key, value, decay, rate, key_gain, decay_bias, shift, extra):
    tok_rows, width = receptance.shape
    chunks, pairs = tok_rows // CHUNK, width // PAIR
    logits = decay + decay_bias + shift
    log_decay = sigmoid(logits) * (-0.6065306597126334) + extra
    scaled = key * key_gain
    ones = group_ones(width)
    unit = scaled * lax.rsqrt(dot2(scaled * scaled, ones) + KEY_EPS)
    erase = unit * sigmoid(rate)
    row, col = iota((tok_rows, tok_rows), 0), iota((tok_rows, tok_rows), 1)
    running = ((row // CHUNK == col // CHUNK) & (row >= col)).astype(BF16)
    high, low = split(log_decay)
    total = dot(running, high) + dot(running, low)

    strict_rows = iota((CHUNK, PAIR), 0)
    strict_cols = iota((CHUNK, PAIR), 1) % HEAD
    strict = strict_rows > strict_cols
    inclusive = strict_rows >= strict_cols
    eye = (strict_rows == strict_cols).astype(F32)
    same8 = (strict_rows // 8) == (strict_cols // 8)
    lane_first = first_head(CHUNK)

    units = []
    for c in range(chunks):
        rows = slice(c * CHUNK, (c + 1) * CHUNK)
        cum = total[rows]
        last = cum[CHUNK - 1 : CHUNK]
        half = 0.5 * last
        grow = jnp.exp(half - cum)
        shrink = jnp.exp(cum - half)
        half_decay = jnp.exp(half)
        query_unit = unit[rows] * jnp.exp(cum - log_decay[rows] - half)
        query_read = receptance[rows] * shrink
        scaled_erase = erase[rows] * grow
        scaled_key = key[rows] * grow
        for p in range(pairs):
            lanes = slice(p * PAIR, (p + 1) * PAIR)
            units.append(
                dict(
                    c=c,
                    p=p,
                    qu=query_unit[:, lanes],
                    qr=query_read[:, lanes],
                    se=scaled_erase[:, lanes],
                    sk=scaled_key[:, lanes],
                    v=value[rows, lanes],
                    half=half_decay[:, lanes],
                )
            )
    for u in units:
        left = jnp.concatenate([u["qu"], u["qr"]], axis=0)
        right = jnp.concatenate([diagonal(u["se"]), diagonal(u["sk"])], axis=0)
        u["gram"] = dot3(left, right, NT)
    for u in units:
        gram = u.pop("gram")
        u["mix"] = jnp.where(strict, gram[:CHUNK, :PAIR], 0.0)
        u["key_mix"] = jnp.where(strict, gram[:CHUNK, PAIR:], 0.0)
        u["read_erase"] = jnp.where(inclusive, gram[CHUNK:, :PAIR], 0.0)
        u["read_key"] = jnp.where(inclusive, gram[CHUNK:, PAIR:], 0.0)
        u["near"] = jnp.where(same8, u["mix"], 0.0)
        u["far"] = jnp.where(same8, 0.0, u["mix"])
    for u in units:
        u["near2"] = dot3(u["near"], diagonal(u["near"]))
        u["value_part"] = dot3(
            jnp.concatenate([u.pop("key_mix"), u.pop("read_key")], axis=0), diagonal(u["v"])
        )
    for u in units:
        powers = dot3(jnp.concatenate([u["near"], u["near2"]], axis=0), diagonal(u["near2"]))
        u["start"] = eye - u.pop("near") + u.pop("near2") - powers[:CHUNK]
        u["near4"] = powers[CHUNK:]
    for u in units:
        u["inv8"] = u["start"] + dot3(u["start"], diagonal(u.pop("near4")))
        u.pop("start")
    for u in units:
        u["step"] = dot3(u["inv8"], diagonal(u.pop("far")))
    for u in units:
        out = dot3(u["step"], beside(diagonal(u["step"]), diagonal(u["inv8"])))
        u["step2"] = out[:, :PAIR]
        u["inv"] = u.pop("inv8") - out[:, PAIR:]
        u.pop("step")
    for u in units:
        out = dot3(u["step2"], beside(diagonal(u["step2"]), diagonal(u["inv"])))
        u["step4"] = out[:, :PAIR]
        u["inv"] = u["inv"] + out[:, PAIR:]
        u.pop("step2")
    for u in units:
        u["inv"] = u["inv"] + dot3(u.pop("step4"), diagonal(u["inv"]))
    for u in units:
        right = beside(diagonal(u["value_part"][:CHUNK]), diagonal(u["qu"] * u["half"]))
        u["removed"] = -dot3(u.pop("inv"), right)
    for u in units:
        kept = jnp.concatenate([u["se"] * u["half"], u["sk"] * u["half"]], axis=0)
        right = jnp.concatenate(
            [u["removed"], beside(u["v"], jnp.zeros_like(u["v"]))], axis=0
        )
        out = dot3(kept.T, right)
        u["base"] = undiagonal(out[:, :PAIR])
        u["trans"] = undiagonal(out[:, PAIR:]) + eye * (u["half"] * u["half"])
    for u in units:
        removed = u["removed"]
        right = beside(diagonal(removed[:, :PAIR]), diagonal(removed[:, PAIR:]))
        out = dot3(u["read_erase"], right)
        u["local"] = out[:, :PAIR] + u["value_part"][CHUNK:]
        u["carried"] = out[:, PAIR:] + u["qr"] * u["half"]
    return units


def chunk_prefixes(units, pairs, chunks):
    found = []
    for p in range(pairs):
        steps = [(u["trans"], u["base"]) for u in units if u["p"] == p]
        one = steps[0]
        two = compose(steps[1], one, dot3)
        upper = compose(steps[3], steps[2], dot3)
        three = compose(steps[2], two, dot3)
        found.append([one, two, three, compose(upper, two, dot3)])
    return found


def local_kernel(
    tokens_hbm, gain_ref, decay_hbm, key_hbm, rate_hbm, receptance_hbm, value_hbm,
    key_gain_ref, bias_ref, shift_hbm, extra_hbm,
    normed_hbm, total_ref, prefix_ref, local_ref, carried_ref,
    tokens, normed, weights, shift, extra, sems,
):
    order = (decay_hbm, key_hbm, rate_hbm, receptance_hbm, value_hbm)
    copies = [pltpu.make_async_copy(tokens_hbm, tokens, sems.at[0])]
    for i, source in enumerate(order):
        copies.append(pltpu.make_async_copy(source, weights.at[i], sems.at[1 + i]))
    copies.append(pltpu.make_async_copy(shift_hbm, shift, sems.at[6]))
    copies.append(pltpu.make_async_copy(extra_hbm, extra, sems.at[7]))
    for copy in copies:
        copy.start()
    copies[0].wait()
    normed[...] = normalize(tokens[...], gain_ref[...])
    out_copy = pltpu.make_async_copy(normed, normed_hbm, sems.at[8])
    out_copy.start()
    found = []
    for i in range(5):
        copies[1 + i].wait()
        found.append(rounded(dot(normed[...], weights[i])))
    decay, key, rate, receptance, value = found
    copies[6].wait()
    copies[7].wait()
    units = chunk_algebra(
        receptance, key, value, decay, rate, key_gain_ref[...], bias_ref[...], shift[...], extra[...]
    )
    chunks, pairs = 4, 2
    prefixes = chunk_prefixes(units, pairs, chunks)
    for p in range(pairs):
        total_ref[p] = beside(*prefixes[p][3])
        for k in range(3):
            prefix_ref[p, k] = beside(*prefixes[p][k])
    for u in units:
        rows = slice(u["c"] * CHUNK, (u["c"] + 1) * CHUNK)
        lanes = slice(u["p"] * PAIR, (u["p"] + 1) * PAIR)
        local_ref[rows, lanes] = u["local"]
        carried_ref[rows, lanes] = u["carried"]
    out_copy.wait()


def finish_kernel(
    total_ref, prefix_ref, local_ref, carried_ref, normed_hbm,
    conv_value_hbm, conv_gate_hbm, gate_hbm, taps_ref, group_gain_ref, group_shift_ref,
    head_gain_ref, conv_out_hbm, mix_out_hbm,
    out_ref,
    normed, conv_w, gate_w, conv_out_w, mix_out_w,
    peer_total, pair_states, y_slots, z_slots, extended, halo, conv_rows, mix_rows,
    conv_full, mix_full, acc,
    load_sems, pair_send, pair_recv, y_send, y_recv, z_send, z_recv, halo_send, halo_recv,
    conv_send, conv_recv, mix_send, mix_recv,
):
    sp, tp = lax.axis_index("sp"), lax.axis_index("tp")
    core = lax.rem(sp, 2)
    y = lax.rem(sp // 2, 4)
    z = sp // 8
    sibling = sp + 1 - 2 * core
    after, before = lax.rem(sp + 1, 32), lax.rem(sp + 31, 32)

    def y_of(step):
        return lax.rem(y + step, 4)

    def z_of(step):
        return lax.rem(z + step, 4)

    def x_of(step):
        return lax.rem(tp + step, 4)

    def y_peer(step):
        return (z * 8 + y_of(step) * 2 + core, tp)

    def z_peer(step):
        return (z_of(step) * 8 + y * 2 + core, tp)

    def x_peer(step):
        return (sp, x_of(step))

    loads = [
        pltpu.make_async_copy(normed_hbm, normed, load_sems.at[0]),
        pltpu.make_async_copy(conv_value_hbm, conv_w.at[0], load_sems.at[1]),
        pltpu.make_async_copy(conv_gate_hbm, conv_w.at[1], load_sems.at[2]),
        pltpu.make_async_copy(gate_hbm, gate_w, load_sems.at[3]),
        pltpu.make_async_copy(conv_out_hbm, conv_out_w, load_sems.at[4]),
        pltpu.make_async_copy(mix_out_hbm, mix_out_w, load_sems.at[5]),
    ]
    for load in loads:
        load.start()

    barrier = pltpu.get_barrier_semaphore()
    peers = [(sibling, tp), (after, tp), (before, tp)]
    for step in (1, 2, 3):
        peers += [y_peer(step), z_peer(step), x_peer(step)]
    for peer in peers:
        pl.semaphore_signal(barrier, inc=1, device_id=peer, device_id_type=MESH)
    pl.semaphore_wait(barrier, len(peers))

    def remote(source, target, send, recv, peer):
        return pltpu.make_async_remote_copy(
            src_ref=source, dst_ref=target, send_sem=send, recv_sem=recv,
            device_id=peer, device_id_type=MESH,
        )

    pair_copy = remote(
        total_ref.at[1 - core], peer_total, pair_send.at[0], pair_recv.at[0], (sibling, tp)
    )
    pair_copy.start()

    loads[0].wait()
    loads[1].wait()
    conv_value = rounded(dot(normed[...], conv_w[0]))
    loads[2].wait()
    conv_gate = rounded(dot(normed[...], conv_w[1]))
    conv_input = (conv_value * sigmoid(conv_gate)).astype(BF16)
    conv_rows[...] = conv_input[224:]
    halo_copy = remote(conv_rows, halo, halo_send.at[0], halo_recv.at[0], (after, tp))
    halo_copy.start()
    extended[32:, :] = conv_input.astype(F32)

    pair_copy.wait()
    own, other = total_ref[core], peer_total[...]
    is_first = core == 0
    first = jnp.where(is_first, own, other)
    second = jnp.where(is_first, other, own)
    chip_first = (first[:, :PAIR], first[:, PAIR:])
    chip = compose((second[:, :PAIR], second[:, PAIR:]), chip_first, dot3)
    y_slots[y] = beside(*chip).astype(BF16)
    y_copies = []
    for step in (1, 2, 3):
        copy = remote(
            y_slots.at[y], y_slots.at[y], y_send.at[step - 1], y_recv.at[step - 1], y_peer(step)
        )
        copy.start()
        y_copies.append(copy)

    loads[3].wait()
    out_gate = sigmoid(rounded(dot(normed[...], gate_w[...])))
    gate_gain = out_gate * head_gain_ref[...]
    local_rows, carried_rows = [], []
    for p in range(2):
        lanes = slice(p * PAIR, (p + 1) * PAIR)
        local_parts, carried_parts = [local_ref[:CHUNK, lanes]], [carried_ref[:CHUNK, lanes]]
        for c in range(1, 4):
            rows = slice(c * CHUNK, (c + 1) * CHUNK)
            earlier = prefix_ref[p, c - 1]
            out = dot3(
                carried_ref[rows, lanes],
                beside(diagonal(earlier[:, :PAIR]), diagonal(earlier[:, PAIR:])),
            )
            carried_parts.append(out[:, :PAIR])
            local_parts.append(out[:, PAIR:] + local_ref[rows, lanes])
        local_rows.append(jnp.concatenate(local_parts, axis=0))
        carried_rows.append(jnp.concatenate(carried_parts, axis=0))

    for step in (1, 2, 3):
        copy = y_copies[step - 1]
        copy.wait_send()
        arrived = y_of(4 - step)
        remote(
            y_slots.at[arrived], y_slots.at[arrived], y_send.at[step - 1], y_recv.at[step - 1],
            y_peer(step),
        ).wait_recv()

    def slot(ref, k):
        both = ref[k].astype(F32)
        return both[:, :PAIR], both[:, PAIR:]

    c0, c1, c2, c3 = (slot(y_slots, k) for k in range(4))
    c01, c23 = compose(c1, c0, dot1), compose(c3, c2, dot1)
    plane = compose(c23, c01, dot3)
    z_slots[z] = beside(*plane).astype(BF16)
    z_copies = []
    for step in (1, 2, 3):
        copy = remote(
            z_slots.at[z], z_slots.at[z], z_send.at[step - 1], z_recv.at[step - 1], z_peer(step)
        )
        copy.start()
        z_copies.append(copy)
    c012 = compose(c2, c01, dot3)
    eye = (iota((HEAD, PAIR), 0) == iota((HEAD, PAIR), 1) % HEAD).astype(F32)

    def pick(index, a, b, c, d):
        return jnp.where(index == 0, a, jnp.where(index == 1, b, jnp.where(index == 2, c, d)))

    before_chip = (
        pick(y, eye, c0[0], c01[0], c012[0]),
        pick(y, jnp.zeros_like(eye), c0[1], c01[1], c012[1]),
    )
    before_second = compose(chip_first, before_chip, dot3)
    trans_both = jnp.concatenate([before_chip[0], before_second[0]], axis=0)
    base_both = jnp.concatenate([before_chip[1], before_second[1]], axis=0)

    halo_copy.wait()
    extended[:32, :] = jnp.where(sp == 0, 0.0, halo[...].astype(F32))
    taps = taps_ref[...]
    conv_sum = jnp.zeros((256, PAIR), F32)
    for j in range(31):
        conv_sum = conv_sum + taps[j : j + 1] * extended[pl.ds(2 + j, 256), :]
    ones_pair = group_ones(PAIR)
    affine = group_norm(conv_sum, ones_pair, GROUP_EPS) * group_gain_ref[...] + group_shift_ref[...]
    conv_out = (affine * sigmoid(affine)).astype(BF16)
    for k in range(4):
        conv_full[0, k] = conv_out[k * 64 : (k + 1) * 64]
    conv_copies = []
    for step in (1, 2, 3):
        copy = remote(
            conv_full.at[0, x_of(step)], conv_full.at[1, tp],
            conv_send.at[step - 1], conv_recv.at[step - 1], x_peer(step),
        )
        copy.start()
        conv_copies.append(copy)

    for step in (1, 2, 3):
        z_copies[step - 1].wait_send()
        arrived = z_of(4 - step)
        remote(
            z_slots.at[arrived], z_slots.at[arrived], z_send.at[step - 1], z_recv.at[step - 1],
            z_peer(step),
        ).wait_recv()
    p0, p1, p2 = (slot(z_slots, k) for k in range(3))
    into1 = p0[1]
    into2 = dot1(p1[0], diagonal(into1)) + p1[1]
    into3 = dot3(p2[0], diagonal(into2)) + p2[1]
    entering = pick(z, jnp.zeros_like(into1), into1, into2, into3)
    states = dot3(trans_both, diagonal(entering)) + base_both
    state_first, state_second = states[:HEAD], states[HEAD:]
    mine = jnp.where(is_first, state_first, state_second)
    pair_states[0] = jnp.where(is_first, state_second, state_first)
    state_copy = remote(
        pair_states.at[0], pair_states.at[1], pair_send.at[1], pair_recv.at[1], (sibling, tp)
    )
    state_copy.start()

    loads[4].wait()
    acc[...] = dot(conv_full[0, tp], conv_out_w[pl.ds(pl.multiple_of(tp * PAIR, PAIR), PAIR), :])
    for step in (1, 2, 3):
        conv_copies[step - 1].wait_send()
        arrived = x_of(4 - step)
        remote(
            conv_full.at[0, arrived], conv_full.at[1, arrived],
            conv_send.at[step - 1], conv_recv.at[step - 1], x_peer(step),
        ).wait_recv()
        rows = pl.ds(pl.multiple_of(arrived * PAIR, PAIR), PAIR)
        acc[...] += dot(conv_full[1, arrived], conv_out_w[rows, :])

    state_copy.wait()
    theirs = pair_states[1]
    state_pairs = (jnp.where(is_first, mine, theirs), jnp.where(is_first, theirs, mine))
    readout = beside(
        *(local_rows[p] + dot3(carried_rows[p], diagonal(state_pairs[p])) for p in range(2))
    )
    mix_out = (group_norm(readout, group_ones(256), HEAD_EPS) * gate_gain).astype(BF16)
    for k in range(4):
        mix_full[0, k] = mix_out[k * 64 : (k + 1) * 64]
    mix_copies = []
    for step in (1, 2, 3):
        copy = remote(
            mix_full.at[0, x_of(step)], mix_full.at[1, tp],
            mix_send.at[step - 1], mix_recv.at[step - 1], x_peer(step),
        )
        copy.start()
        mix_copies.append(copy)
    loads[5].wait()
    acc[...] += dot(mix_full[0, tp], mix_out_w[pl.ds(pl.multiple_of(tp * 256, 256), 256), :])
    for step in (1, 3, 2):
        mix_copies[step - 1].wait_send()
        arrived = x_of(4 - step)
        remote(
            mix_full.at[0, arrived], mix_full.at[1, arrived],
            mix_send.at[step - 1], mix_recv.at[step - 1], x_peer(step),
        ).wait_recv()
        rows = pl.ds(pl.multiple_of(arrived * 256, 256), 256)
        acc[...] += dot(mix_full[1, arrived], mix_out_w[rows, :])
    out_ref[...] = acc[...].astype(BF16)


VMEM = pl.BlockSpec(memory_space=pltpu.VMEM)
ANY = pl.BlockSpec(memory_space=pl.ANY)


def local(
    tokens, input_norm_gain, convolution_value_weight, convolution_gate_weight,
    depthwise_taps_weight, convolution_group_gain, convolution_group_shift, receptance_weight,
    key_weight, value_weight, decay_weight, correction_rate_weight, output_gate_weight,
    key_prenorm_gain, decay_offset_bias, position_decay_shift, extra_log_decay, head_norm_gain,
    convolution_output_weight, attention_output_weight,
):
    normed, total, prefix, local_read, carried = pl.pallas_call(
        local_kernel,
        name="local_part",
        out_shape=(
            jax.ShapeDtypeStruct((256, 2048), BF16),
            jax.ShapeDtypeStruct((2, 64, 256), F32),
            jax.ShapeDtypeStruct((2, 3, 64, 256), F32),
            jax.ShapeDtypeStruct((256, 256), F32),
            jax.ShapeDtypeStruct((256, 256), F32),
        ),
        in_specs=[ANY, VMEM, ANY, ANY, ANY, ANY, ANY, VMEM, VMEM, ANY, ANY],
        out_specs=(ANY, VMEM, VMEM, VMEM, VMEM),
        scratch_shapes=[
            pltpu.VMEM((256, 2048), BF16),
            pltpu.VMEM((256, 2048), BF16),
            pltpu.VMEM((5, 2048, 256), BF16),
            pltpu.VMEM((256, 256), F32),
            pltpu.VMEM((256, 256), F32),
            pltpu.SemaphoreType.DMA((9,)),
        ],
    )(
        tokens, input_norm_gain.reshape(1, -1), decay_weight, key_weight, correction_rate_weight,
        receptance_weight, value_weight, key_prenorm_gain.reshape(1, -1),
        decay_offset_bias.reshape(1, -1), position_decay_shift, extra_log_decay,
    )
    dma = pltpu.SemaphoreType.DMA
    return pl.pallas_call(
        finish_kernel,
        name="finish_part",
        out_shape=jax.ShapeDtypeStruct((64, 2048), BF16),
        in_specs=[VMEM, VMEM, VMEM, VMEM, ANY, ANY, ANY, ANY, VMEM, VMEM, VMEM, VMEM, ANY, ANY],
        out_specs=VMEM,
        scratch_shapes=[
            pltpu.VMEM((256, 2048), BF16),
            pltpu.VMEM((2, 2048, 128), BF16),
            pltpu.VMEM((2048, 256), BF16),
            pltpu.VMEM((512, 2048), BF16),
            pltpu.VMEM((1024, 2048), BF16),
            pltpu.VMEM((64, 256), F32),
            pltpu.VMEM((2, 64, 128), F32),
            pltpu.VMEM((4, 64, 256), BF16),
            pltpu.VMEM((4, 64, 256), BF16),
            pltpu.VMEM((288, 128), F32),
            pltpu.VMEM((32, 128), BF16),
            pltpu.VMEM((32, 128), BF16),
            pltpu.VMEM((8, 128), BF16),
            pltpu.VMEM((2, 4, 64, 128), BF16),
            pltpu.VMEM((2, 4, 64, 256), BF16),
            pltpu.VMEM((64, 2048), F32),
            dma((6,)), dma((2,)), dma((2,)), dma((3,)), dma((3,)), dma((3,)), dma((3,)),
            dma((1,)), dma((1,)), dma((3,)), dma((3,)), dma((3,)), dma((3,)),
        ],
        compiler_params=pltpu.CompilerParams(collective_id=0, has_side_effects=True),
    )(
        total, prefix, local_read, carried, normed,
        convolution_value_weight, convolution_gate_weight, output_gate_weight,
        depthwise_taps_weight, convolution_group_gain.reshape(1, -1),
        convolution_group_shift.reshape(1, -1), head_norm_gain.reshape(1, -1),
        convolution_output_weight, attention_output_weight,
    )


def solution(mesh):
    rows, chans, vec = P("sp", None), P(None, "tp"), P("tp")
    placed = (
        rows, P(), chans, chans, chans, vec, vec, chans, chans, chans, chans, chans, chans,
        vec, vec, P("sp", "tp"), P("sp", "tp"), vec, P(), P(),
    )
    return jax.shard_map(
        local, mesh=mesh, in_specs=placed, out_specs=P(("sp", "tp"), None), check_vma=False
    )
```

```python
import functools

import jax
import jax.numpy as jnp
from jax import lax
from jax.experimental import pallas as pl
from jax.experimental.pallas import tpu as pltpu
from jax.sharding import PartitionSpec as P

F32 = jnp.float32
BF16 = jnp.bfloat16
MESH = pl.DeviceIdType.MESH
HEAD = 64
CHUNK = 64
PAIR = 128

NORM_EPS = 1e-06
GROUP_EPS = 1e-05
HEAD_EPS = 0.00064
KEY_EPS = 1e-06

NN = (((1,), (0,)), ((), ()))
NT = (((1,), (1,)), ((), ()))


def dot(left, right, dims=NN):
    return lax.dot_general(left, right, dims, preferred_element_type=F32)


def split(values):
    high = values.astype(BF16)
    return high, (values - high.astype(F32)).astype(BF16)


def dot1(left, right, dims=NN):
    return dot(left.astype(BF16), right.astype(BF16), dims)


def dot3(left, right, dims=NN):
    left_high, left_low = split(left)
    right_high, right_low = split(right)
    return dot(left_high, right_high, dims) + (
        dot(left_low, right_high, dims) + dot(left_high, right_low, dims)
    )


def dot2(left, right_exact):
    high, low = split(left)
    return dot(high, right_exact) + dot(low, right_exact)


def iota(shape, dim):
    return lax.broadcasted_iota(jnp.int32, shape, dim)


def first_head(rows):
    return iota((rows, PAIR), 1) < HEAD


def diagonal(packed):
    mask = first_head(packed.shape[0])
    return jnp.concatenate([jnp.where(mask, packed, 0.0), jnp.where(mask, 0.0, packed)], axis=0)


def undiagonal(full):
    return jnp.where(first_head(HEAD), full[:HEAD], full[HEAD:])


def beside(*parts):
    return jnp.concatenate(parts, axis=1)


def group_ones(width):
    return (iota((width, width), 0) // HEAD == iota((width, width), 1) // HEAD).astype(BF16)


def sigmoid(values):
    return 1.0 / (1.0 + jnp.exp(-values))


def rounded(values):
    return values.astype(BF16).astype(F32)


def normalize(tokens, gain):
    rows = tokens.astype(F32)
    scale = lax.rsqrt(jnp.mean(rows * rows, axis=-1, keepdims=True) + NORM_EPS)
    return (rows * scale * gain).astype(BF16)


def group_norm(values, ones, eps):
    centred = values - dot2(values, ones) * (1.0 / HEAD)
    return centred * lax.rsqrt(dot2(centred * centred, ones) * (1.0 / HEAD) + eps)


def compose(later, earlier, product):
    trans, base = later
    out = product(trans, beside(diagonal(earlier[0]), diagonal(earlier[1])))
    return out[:, :PAIR], out[:, PAIR:] + base


def chunk_algebra(receptance, key, value, decay, rate, key_gain, decay_bias, shift, extra):
    tok_rows, width = receptance.shape
    chunks, pairs = tok_rows // CHUNK, width // PAIR
    logits = decay + decay_bias + shift
    log_decay = sigmoid(logits) * (-0.6065306597126334) + extra
    scaled = key * key_gain
    ones = group_ones(width)
    unit = scaled * lax.rsqrt(dot2(scaled * scaled, ones) + KEY_EPS)
    erase = unit * sigmoid(rate)
    row, col = iota((tok_rows, tok_rows), 0), iota((tok_rows, tok_rows), 1)
    running = ((row // CHUNK == col // CHUNK) & (row >= col)).astype(BF16)
    high, low = split(log_decay)
    total = dot(running, high) + dot(running, low)

    strict_rows = iota((CHUNK, PAIR), 0)
    strict_cols = iota((CHUNK, PAIR), 1) % HEAD
    strict = strict_rows > strict_cols
    inclusive = strict_rows >= strict_cols
    eye = (strict_rows == strict_cols).astype(F32)
    same8 = (strict_rows // 8) == (strict_cols // 8)
    lane_first = first_head(CHUNK)

    units = []
    for c in range(chunks):
        rows = slice(c * CHUNK, (c + 1) * CHUNK)
        cum = total[rows]
        last = cum[CHUNK - 1 : CHUNK]
        half = 0.5 * last
        grow = jnp.exp(half - cum)
        shrink = jnp.exp(cum - half)
        half_decay = jnp.exp(half)
        query_unit = unit[rows] * jnp.exp(cum - log_decay[rows] - half)
        query_read = receptance[rows] * shrink
        scaled_erase = erase[rows] * grow
        scaled_key = key[rows] * grow
        for p in range(pairs):
            lanes = slice(p * PAIR, (p + 1) * PAIR)
            units.append(
                dict(
                    c=c,
                    p=p,
                    qu=query_unit[:, lanes],
                    qr=query_read[:, lanes],
                    se=scaled_erase[:, lanes],
                    sk=scaled_key[:, lanes],
                    v=value[rows, lanes],
                    half=half_decay[:, lanes],
                )
            )
    for u in units:
        left = jnp.concatenate([u["qu"], u["qr"]], axis=0)
        right = jnp.concatenate([diagonal(u["se"]), diagonal(u["sk"])], axis=0)
        u["gram"] = dot3(left, right, NT)
    for u in units:
        gram = u.pop("gram")
        u["mix"] = jnp.where(strict, gram[:CHUNK, :PAIR], 0.0)
        u["key_mix"] = jnp.where(strict, gram[:CHUNK, PAIR:], 0.0)
        u["read_erase"] = jnp.where(inclusive, gram[CHUNK:, :PAIR], 0.0)
        u["read_key"] = jnp.where(inclusive, gram[CHUNK:, PAIR:], 0.0)
        u["near"] = jnp.where(same8, u["mix"], 0.0)
        u["far"] = jnp.where(same8, 0.0, u["mix"])
    for u in units:
        u["near2"] = dot3(u["near"], diagonal(u["near"]))
        u["value_part"] = dot3(
            jnp.concatenate([u.pop("key_mix"), u.pop("read_key")], axis=0), diagonal(u["v"])
        )
    for u in units:
        powers = dot3(jnp.concatenate([u["near"], u["near2"]], axis=0), diagonal(u["near2"]))
        u["start"] = eye - u.pop("near") + u.pop("near2") - powers[:CHUNK]
        u["near4"] = powers[CHUNK:]
    for u in units:
        u["inv8"] = u["start"] + dot3(u["start"], diagonal(u.pop("near4")))
        u.pop("start")
    for u in units:
        u["step"] = dot3(u["inv8"], diagonal(u.pop("far")))
    for u in units:
        out = dot3(u["step"], beside(diagonal(u["step"]), diagonal(u["inv8"])))
        u["step2"] = out[:, :PAIR]
        u["inv"] = u.pop("inv8") - out[:, PAIR:]
        u.pop("step")
    for u in units:
        out = dot3(u["step2"], beside(diagonal(u["step2"]), diagonal(u["inv"])))
        u["step4"] = out[:, :PAIR]
        u["inv"] = u["inv"] + out[:, PAIR:]
        u.pop("step2")
    for u in units:
        u["inv"] = u["inv"] + dot3(u.pop("step4"), diagonal(u["inv"]))
    for u in units:
        right = beside(diagonal(u["value_part"][:CHUNK]), diagonal(u["qu"] * u["half"]))
        u["removed"] = -dot3(u.pop("inv"), right)
    for u in units:
        kept = jnp.concatenate([u["se"] * u["half"], u["sk"] * u["half"]], axis=0)
        right = jnp.concatenate(
            [u["removed"], beside(u["v"], jnp.zeros_like(u["v"]))], axis=0
        )
        out = dot3(kept.T, right)
        u["base"] = undiagonal(out[:, :PAIR])
        u["trans"] = undiagonal(out[:, PAIR:]) + eye * (u["half"] * u["half"])
    return units


def local_reads(units):
    for u in units:
        removed = u["removed"]
        right = beside(diagonal(removed[:, :PAIR]), diagonal(removed[:, PAIR:]))
        out = dot3(u["read_erase"], right)
        u["local"] = out[:, :PAIR] + u["value_part"][CHUNK:]
        u["carried"] = out[:, PAIR:] + u["qr"] * u["half"]


def layer_kernel(
    tokens_hbm, gain_ref, decay_hbm, key_hbm, rate_hbm, receptance_hbm, value_hbm,
    key_gain_ref, bias_ref, shift_hbm, extra_hbm,
    conv_value_hbm, conv_gate_hbm, gate_hbm, taps_ref, group_gain_ref, group_shift_ref,
    head_gain_ref, conv_out_hbm, mix_out_hbm,
    out_ref,
    tokens, normed, weights, shift, extra, conv_w, gate_w, conv_out_w, mix_out_w,
    totals, peer_total, pair_states, y_slots, z_slots, extended, halo, conv_rows,
    local_rows, carried_rows, gate_gain, conv_full, mix_sent, mix_full, acc,
    sems, load_sems, pair_send, pair_recv, y_send, y_recv, z_send, z_recv, halo_send, halo_recv,
    conv_send, conv_recv, mix_send, mix_recv,
):
    sp, tp = lax.axis_index("sp"), lax.axis_index("tp")
    core = lax.rem(sp, 2)
    y = lax.rem(sp // 2, 4)
    z = sp // 8
    sibling = sp + 1 - 2 * core
    after, before = lax.rem(sp + 1, 32), lax.rem(sp + 31, 32)
    is_first = core == 0

    def y_of(step):
        return lax.rem(y + step, 4)

    def z_of(step):
        return lax.rem(z + step, 4)

    def x_of(step):
        return lax.rem(tp + step, 4)

    def y_peer(step):
        return (z * 8 + y_of(step) * 2 + core, tp)

    def z_peer(step):
        return (z_of(step) * 8 + y * 2 + core, tp)

    def x_peer(step):
        return (sp, x_of(step))

    def remote(source, target, send, recv, peer):
        return pltpu.make_async_remote_copy(
            src_ref=source, dst_ref=target, send_sem=send, recv_sem=recv,
            device_id=peer, device_id_type=MESH,
        )

    order = (decay_hbm, key_hbm, rate_hbm, receptance_hbm, value_hbm)
    copies = [pltpu.make_async_copy(tokens_hbm, tokens, sems.at[0])]
    for i, source in enumerate(order):
        copies.append(pltpu.make_async_copy(source, weights.at[i], sems.at[1 + i]))
    copies.append(pltpu.make_async_copy(shift_hbm, shift, sems.at[6]))
    copies.append(pltpu.make_async_copy(extra_hbm, extra, sems.at[7]))
    for copy in copies:
        copy.start()

    barrier = pltpu.get_barrier_semaphore()
    peers = [(sibling, tp), (after, tp), (before, tp)]
    for step in (1, 2, 3):
        peers += [y_peer(step), z_peer(step), x_peer(step)]
    for peer in peers:
        pl.semaphore_signal(barrier, inc=1, device_id=peer, device_id_type=MESH)

    loads = [
        pltpu.make_async_copy(conv_value_hbm, conv_w.at[0], load_sems.at[0]),
        pltpu.make_async_copy(conv_gate_hbm, conv_w.at[1], load_sems.at[1]),
        pltpu.make_async_copy(gate_hbm, gate_w, load_sems.at[2]),
        pltpu.make_async_copy(conv_out_hbm, conv_out_w, load_sems.at[3]),
        pltpu.make_async_copy(mix_out_hbm, mix_out_w, load_sems.at[4]),
    ]
    with jax.named_scope("wait_tokens"):
        copies[0].wait()
    with jax.named_scope("norm"):
        normed[...] = normalize(tokens[...], gain_ref[...])
    with jax.named_scope("project"):
        found = []
        for i in range(5):
            copies[1 + i].wait()
            found.append(rounded(dot(normed[...], weights[i])))
        decay, key, rate, receptance, value = found
        copies[6].wait()
        copies[7].wait()
    for load in loads:
        load.start()
    with jax.named_scope("algebra"):
        units = chunk_algebra(
            receptance, key, value, decay, rate, key_gain_ref[...], bias_ref[...], shift[...],
            extra[...],
        )
    with jax.named_scope("totals"):
        prefixes = []
        for p in range(2):
            steps = [(u["trans"], u["base"]) for u in units if u["p"] == p]
            two = compose(steps[1], steps[0], dot3)
            upper = compose(steps[3], steps[2], dot3)
            totals[p] = beside(*compose(upper, two, dot3))
            prefixes.append((steps[0], two, steps[2]))
    with jax.named_scope("barrier"):
        pl.semaphore_wait(barrier, len(peers))
    pair_copy = remote(
        totals.at[1 - core], peer_total, pair_send.at[0], pair_recv.at[0], (sibling, tp)
    )
    pair_copy.start()

    with jax.named_scope("conv_project"):
        loads[0].wait()
        conv_value = rounded(dot(normed[...], conv_w[0]))
        loads[1].wait()
        conv_gate = rounded(dot(normed[...], conv_w[1]))
        conv_input = (conv_value * sigmoid(conv_gate)).astype(BF16)
        conv_rows[...] = conv_input[224:]
        halo_copy = remote(conv_rows, halo, halo_send.at[0], halo_recv.at[0], (after, tp))
        halo_copy.start()
        extended[32:, :] = conv_input.astype(F32)

    with jax.named_scope("pair_wait"):
        pair_copy.wait()
    with jax.named_scope("pair_compose"):
        own, other = totals[core], peer_total[...]
        first = jnp.where(is_first, own, other)
        second = jnp.where(is_first, other, own)
        chip_first = (first[:, :PAIR], first[:, PAIR:])
        chip = compose((second[:, :PAIR], second[:, PAIR:]), chip_first, dot3)
        y_slots[y] = beside(*chip).astype(BF16)
    y_copies = []
    for step in (2, 1, 3):
        copy = remote(
            y_slots.at[y], y_slots.at[y], y_send.at[step - 1], y_recv.at[step - 1], y_peer(step)
        )
        copy.start()
        y_copies.append(copy)

    with jax.named_scope("gate_project"):
        loads[2].wait()
        gated = sigmoid(rounded(dot(normed[...], gate_w[...]))) * head_gain_ref[...]
        gate_gain[0] = gated[:, :PAIR]
        gate_gain[1] = gated[:, PAIR:]
    with jax.named_scope("local_reads"):
        local_reads(units)
        for p in range(2):
            one, two, third = prefixes[p]
            earlier = (None, one, two, compose(third, two, dot3))
            for u in units:
                if u["p"] != p:
                    continue
                c = u["c"]
                rows = slice(c * CHUNK, (c + 1) * CHUNK)
                if c == 0:
                    local_rows[p, rows] = u["local"]
                    carried_rows[p, rows] = u["carried"]
                    continue
                right = beside(diagonal(earlier[c][0]), diagonal(earlier[c][1]))
                out = dot3(u["carried"], right)
                carried_rows[p, rows] = out[:, :PAIR]
                local_rows[p, rows] = out[:, PAIR:] + u["local"]

    with jax.named_scope("y_wait"):
        for copy in y_copies:
            copy.wait_send()
        for step in (1, 3, 2):
            arrived = y_of(4 - step)
            remote(
                y_slots.at[arrived], y_slots.at[arrived], y_send.at[step - 1],
                y_recv.at[step - 1], y_peer(step),
            ).wait_recv()

    def slot(ref, k):
        both = ref[k].astype(F32)
        return both[:, :PAIR], both[:, PAIR:]

    with jax.named_scope("y_compose"):
        c0, c1, c2, c3 = (slot(y_slots, k) for k in range(4))
        c01, c23 = compose(c1, c0, dot1), compose(c3, c2, dot1)
        plane = compose(c23, c01, dot3)
        z_slots[z] = beside(*plane).astype(BF16)
    z_copies = []
    for step in (2, 1, 3):
        copy = remote(
            z_slots.at[z], z_slots.at[z], z_send.at[step - 1], z_recv.at[step - 1], z_peer(step)
        )
        copy.start()
        z_copies.append(copy)
    eye = (iota((HEAD, PAIR), 0) == iota((HEAD, PAIR), 1) % HEAD).astype(F32)
    nothing = jnp.zeros((HEAD, PAIR), F32)

    def pick(index, a, b, c, d):
        return jnp.where(index == 0, a, jnp.where(index == 1, b, jnp.where(index == 2, c, d)))

    with jax.named_scope("before_chip"):
        c012 = compose(c2, c01, dot3)
        before_chip = (
            pick(y, eye, c0[0], c01[0], c012[0]), pick(y, nothing, c0[1], c01[1], c012[1])
        )
        before_second = compose(chip_first, before_chip, dot3)
        trans_both = jnp.concatenate([before_chip[0], before_second[0]], axis=0)
        base_both = jnp.concatenate([before_chip[1], before_second[1]], axis=0)

    with jax.named_scope("halo_wait"):
        halo_copy.wait()
    with jax.named_scope("convolution"):
        extended[:32, :] = jnp.where(sp == 0, 0.0, halo[...].astype(F32))
        taps = taps_ref[...]
        conv_sum = jnp.zeros((256, PAIR), F32)
        for j in range(31):
            conv_sum = conv_sum + taps[j : j + 1] * extended[pl.ds(2 + j, 256), :]
        normal = group_norm(conv_sum, group_ones(PAIR), GROUP_EPS)
        affine = normal * group_gain_ref[...] + group_shift_ref[...]
        conv_out = (affine * sigmoid(affine)).astype(BF16)
        for k in range(4):
            conv_full[0, k] = conv_out[k * 64 : (k + 1) * 64]
    conv_copies = []
    for step in (2, 1, 3):
        copy = remote(
            conv_full.at[0, x_of(step)], conv_full.at[1, tp],
            conv_send.at[step - 1], conv_recv.at[step - 1], x_peer(step),
        )
        copy.start()
        conv_copies.append(copy)

    with jax.named_scope("z_wait"):
        for copy in z_copies:
            copy.wait_send()
        for step in (1, 3, 2):
            arrived = z_of(4 - step)
            remote(
                z_slots.at[arrived], z_slots.at[arrived], z_send.at[step - 1],
                z_recv.at[step - 1], z_peer(step),
            ).wait_recv()
    with jax.named_scope("z_compose"):
        p0, p1, p2 = (slot(z_slots, k) for k in range(3))
        into2 = dot1(p1[0], diagonal(p0[1])) + p1[1]
        last_trans = pick(z, eye, eye, p1[0], p2[0])
        last_base = pick(z, nothing, nothing, p1[1], p2[1])
        inner = pick(z, nothing, p0[1], p0[1], into2)
        out = dot3(trans_both, beside(diagonal(last_trans), diagonal(last_base)))
        states = dot3(out[:, :PAIR], diagonal(inner)) + (out[:, PAIR:] + base_both)
        state_first, state_second = states[:HEAD], states[HEAD:]
        mine = jnp.where(is_first, state_first, state_second)
        pair_states[0] = jnp.where(is_first, state_second, state_first)
    state_copy = remote(
        pair_states.at[0], pair_states.at[1], pair_send.at[1], pair_recv.at[1], (sibling, tp)
    )
    state_copy.start()

    ones = group_ones(PAIR)

    def read_pair(p, state, half):
        readout = local_rows[p] + dot3(carried_rows[p], diagonal(state))
        mix_out = (group_norm(readout, ones, HEAD_EPS) * gate_gain[p]).astype(BF16)
        started = []
        for k in range(4):
            mix_sent[half, k] = mix_out[k * 64 : (k + 1) * 64]
        for step in (2, 1, 3):
            copy = remote(
                mix_sent.at[half, x_of(step)], mix_full.at[half, tp],
                mix_send.at[half, step - 1], mix_recv.at[half, step - 1], x_peer(step),
            )
            copy.start()
            started.append(copy)
        return started

    def out_rows(owner, p):
        return pl.ds(pl.multiple_of(owner * 256 + p * PAIR, PAIR), PAIR)

    with jax.named_scope("read_own"):
        started = read_pair(core, mine, 0)

    with jax.named_scope("conv_project_out"):
        loads[3].wait()
        acc[...] = dot(conv_full[0, tp], conv_out_w[pl.ds(pl.multiple_of(tp * PAIR, PAIR), PAIR), :])
        for copy in conv_copies:
            copy.wait_send()
        for step in (1, 3, 2):
            arrived = x_of(4 - step)
            remote(
                conv_full.at[0, arrived], conv_full.at[1, arrived],
                conv_send.at[step - 1], conv_recv.at[step - 1], x_peer(step),
            ).wait_recv()
            rows = pl.ds(pl.multiple_of(arrived * PAIR, PAIR), PAIR)
            acc[...] += dot(conv_full[1, arrived], conv_out_w[rows, :])
    with jax.named_scope("state_wait"):
        state_copy.wait()
    with jax.named_scope("read_other"):
        started += read_pair(1 - core, pair_states[1], 1)
    with jax.named_scope("mix_own"):
        loads[4].wait()
        acc[...] += dot(mix_sent[0, tp], mix_out_w[out_rows(tp, core), :]) + dot(
            mix_sent[1, tp], mix_out_w[out_rows(tp, 1 - core), :]
        )
        for copy in started:
            copy.wait_send()
    for half in (0, 1):
        for step in (1, 3, 2):
            arrived = x_of(4 - step)
            with jax.named_scope("mix_wait"):
                remote(
                    mix_sent.at[half, arrived], mix_full.at[half, arrived],
                    mix_send.at[half, step - 1], mix_recv.at[half, step - 1], x_peer(step),
                ).wait_recv()
            with jax.named_scope("mix_project"):
                p = core if half == 0 else 1 - core
                acc[...] += dot(mix_full[half, arrived], mix_out_w[out_rows(arrived, p), :])
    out_ref[...] = acc[...].astype(BF16)


VMEM = pl.BlockSpec(memory_space=pltpu.VMEM)
ANY = pl.BlockSpec(memory_space=pltpu.HBM)


def local(
    tokens, input_norm_gain, convolution_value_weight, convolution_gate_weight,
    depthwise_taps_weight, convolution_group_gain, convolution_group_shift, receptance_weight,
    key_weight, value_weight, decay_weight, correction_rate_weight, output_gate_weight,
    key_prenorm_gain, decay_offset_bias, position_decay_shift, extra_log_decay, head_norm_gain,
    convolution_output_weight, attention_output_weight,
):
    dma = pltpu.SemaphoreType.DMA
    return pl.pallas_call(
        layer_kernel,
        name="layer",
        out_shape=jax.ShapeDtypeStruct((64, 2048), BF16),
        in_specs=[ANY, VMEM] + [ANY] * 5 + [VMEM, VMEM] + [ANY] * 5 + [VMEM] * 4 + [ANY] * 2,
        out_specs=VMEM,
        scratch_shapes=[
            pltpu.VMEM((256, 2048), BF16),
            pltpu.VMEM((256, 2048), BF16),
            pltpu.VMEM((5, 2048, 256), BF16),
            pltpu.VMEM((256, 256), F32),
            pltpu.VMEM((256, 256), F32),
            pltpu.VMEM((2, 2048, 128), BF16),
            pltpu.VMEM((2048, 256), BF16),
            pltpu.VMEM((512, 2048), BF16),
            pltpu.VMEM((1024, 2048), BF16),
            pltpu.VMEM((2, 64, 256), F32),
            pltpu.VMEM((64, 256), F32),
            pltpu.VMEM((2, 64, 128), F32),
            pltpu.VMEM((4, 64, 256), BF16),
            pltpu.VMEM((4, 64, 256), BF16),
            pltpu.VMEM((288, 128), F32),
            pltpu.VMEM((32, 128), BF16),
            pltpu.VMEM((32, 128), BF16),
            pltpu.VMEM((2, 256, 128), F32),
            pltpu.VMEM((2, 256, 128), F32),
            pltpu.VMEM((2, 256, 128), F32),
            pltpu.VMEM((2, 4, 64, 128), BF16),
            pltpu.VMEM((2, 4, 64, 128), BF16),
            pltpu.VMEM((2, 4, 64, 128), BF16),
            pltpu.VMEM((64, 2048), F32),
            dma((8,)), dma((5,)), dma((2,)), dma((2,)), dma((3,)), dma((3,)), dma((3,)), dma((3,)),
            dma((1,)), dma((1,)), dma((3,)), dma((3,)), dma((2, 3)), dma((2, 3)),
        ],
        compiler_params=pltpu.CompilerParams(
            collective_id=0, has_side_effects=True, vmem_limit_bytes=66650000
        ),
    )(
        tokens, input_norm_gain.reshape(1, -1), decay_weight, key_weight, correction_rate_weight,
        receptance_weight, value_weight, key_prenorm_gain.reshape(1, -1),
        decay_offset_bias.reshape(1, -1), position_decay_shift, extra_log_decay,
        convolution_value_weight, convolution_gate_weight, output_gate_weight,
        depthwise_taps_weight, convolution_group_gain.reshape(1, -1),
        convolution_group_shift.reshape(1, -1), head_norm_gain.reshape(1, -1),
        convolution_output_weight, attention_output_weight,
    )


def solution(mesh):
    rows, chans, vec = P("sp", None), P(None, "tp"), P("tp")
    placed = (
        rows, P(), chans, chans, chans, vec, vec, chans, chans, chans, chans, chans, chans,
        vec, vec, P("sp", "tp"), P("sp", "tp"), vec, P(), P(),
    )
    return jax.shard_map(
        local, mesh=mesh, in_specs=placed, out_specs=P(("sp", "tp"), None), check_vma=False
    )
```

```python
import functools

import jax
import jax.numpy as jnp
from jax import lax
from jax.experimental import pallas as pl
from jax.experimental.pallas import tpu as pltpu
from jax.sharding import PartitionSpec as P

F32 = jnp.float32
BF16 = jnp.bfloat16
MESH = pl.DeviceIdType.MESH
HEAD = 64
CHUNK = 64
PAIR = 128

NORM_EPS = 1e-06
GROUP_EPS = 1e-05
HEAD_EPS = 0.00064
KEY_EPS = 1e-06

NN = (((1,), (0,)), ((), ()))
NT = (((1,), (1,)), ((), ()))


def dot(left, right, dims=NN):
    return lax.dot_general(left, right, dims, preferred_element_type=F32)


def split(values):
    high = values.astype(BF16)
    return high, (values - high.astype(F32)).astype(BF16)


def dot1(left, right, dims=NN):
    return dot(left.astype(BF16), right.astype(BF16), dims)


def dot3(left, right, dims=NN):
    left_high, left_low = split(left)
    right_high, right_low = split(right)
    return dot(left_high, right_high, dims) + (
        dot(left_low, right_high, dims) + dot(left_high, right_low, dims)
    )


def dot2(left, right_exact):
    high, low = split(left)
    return dot(high, right_exact) + dot(low, right_exact)


def iota(shape, dim):
    return lax.broadcasted_iota(jnp.int32, shape, dim)


def first_head(rows):
    return iota((rows, PAIR), 1) < HEAD


def diagonal(packed):
    mask = first_head(packed.shape[0])
    return jnp.concatenate([jnp.where(mask, packed, 0.0), jnp.where(mask, 0.0, packed)], axis=0)


def undiagonal(full):
    return jnp.where(first_head(HEAD), full[:HEAD], full[HEAD:])


def beside(*parts):
    return jnp.concatenate(parts, axis=1)


def group_ones(width):
    return (iota((width, width), 0) // HEAD == iota((width, width), 1) // HEAD).astype(BF16)


def sigmoid(values):
    return 1.0 / (1.0 + jnp.exp(-values))


def rounded(values):
    return values.astype(BF16).astype(F32)


def normalize(tokens, gain):
    rows = tokens.astype(F32)
    scale = lax.rsqrt(jnp.mean(rows * rows, axis=-1, keepdims=True) + NORM_EPS)
    return (rows * scale * gain).astype(BF16)


def group_norm(values, ones, eps):
    centred = values - dot2(values, ones) * (1.0 / HEAD)
    return centred * lax.rsqrt(dot2(centred * centred, ones) * (1.0 / HEAD) + eps)


def compose(later, earlier, product):
    trans, base = later
    out = product(trans, beside(diagonal(earlier[0]), diagonal(earlier[1])))
    return out[:, :PAIR], out[:, PAIR:] + base


def chunk_algebra(receptance, key, value, decay, rate, key_gain, decay_bias, shift, extra):
    tok_rows, width = receptance.shape
    chunks, pairs = tok_rows // CHUNK, width // PAIR
    logits = decay + decay_bias + shift
    log_decay = sigmoid(logits) * (-0.6065306597126334) + extra
    scaled = key * key_gain
    ones = group_ones(width)
    unit = scaled * lax.rsqrt(dot2(scaled * scaled, ones) + KEY_EPS)
    erase = unit * sigmoid(rate)
    row, col = iota((tok_rows, tok_rows), 0), iota((tok_rows, tok_rows), 1)
    running = ((row // CHUNK == col // CHUNK) & (row >= col)).astype(BF16)
    high, low = split(log_decay)
    total = dot(running, high) + dot(running, low)

    strict_rows = iota((CHUNK, PAIR), 0)
    strict_cols = iota((CHUNK, PAIR), 1) % HEAD
    strict = strict_rows > strict_cols
    inclusive = strict_rows >= strict_cols
    eye = (strict_rows == strict_cols).astype(F32)
    same8 = (strict_rows // 8) == (strict_cols // 8)
    lane_first = first_head(CHUNK)

    units = []
    for c in range(chunks):
        rows = slice(c * CHUNK, (c + 1) * CHUNK)
        cum = total[rows]
        last = cum[CHUNK - 1 : CHUNK]
        half = 0.5 * last
        grow = jnp.exp(half - cum)
        shrink = jnp.exp(cum - half)
        half_decay = jnp.exp(half)
        query_unit = unit[rows] * jnp.exp(cum - log_decay[rows] - half)
        query_read = receptance[rows] * shrink
        scaled_erase = erase[rows] * grow
        scaled_key = key[rows] * grow
        for p in range(pairs):
            lanes = slice(p * PAIR, (p + 1) * PAIR)
            units.append(
                dict(
                    c=c,
                    p=p,
                    qu=query_unit[:, lanes],
                    qr=query_read[:, lanes],
                    se=scaled_erase[:, lanes],
                    sk=scaled_key[:, lanes],
                    v=value[rows, lanes],
                    half=half_decay[:, lanes],
                )
            )
    for u in units:
        left = jnp.concatenate([u["qu"], u["qr"]], axis=0)
        right = jnp.concatenate([diagonal(u["se"]), diagonal(u["sk"])], axis=0)
        u["gram"] = dot1(left, right, NT)
    for u in units:
        gram = u.pop("gram")
        u["mix"] = jnp.where(strict, gram[:CHUNK, :PAIR], 0.0)
        u["key_mix"] = jnp.where(strict, gram[:CHUNK, PAIR:], 0.0)
        u["read_erase"] = jnp.where(inclusive, gram[CHUNK:, :PAIR], 0.0)
        u["read_key"] = jnp.where(inclusive, gram[CHUNK:, PAIR:], 0.0)
        u["near"] = jnp.where(same8, u["mix"], 0.0)
        u["far"] = jnp.where(same8, 0.0, u["mix"])
    for u in units:
        u["near2"] = dot3(u["near"], diagonal(u["near"]))
        u["value_part"] = dot1(
            jnp.concatenate([u.pop("key_mix"), u.pop("read_key")], axis=0), diagonal(u["v"])
        )
    for u in units:
        powers = dot3(jnp.concatenate([u["near"], u["near2"]], axis=0), diagonal(u["near2"]))
        u["start"] = eye - u.pop("near") + u.pop("near2") - powers[:CHUNK]
        u["near4"] = powers[CHUNK:]
    for u in units:
        u["inv8"] = u["start"] + dot3(u["start"], diagonal(u.pop("near4")))
        u.pop("start")
    for u in units:
        u["step"] = dot3(u["inv8"], diagonal(u.pop("far")))
    for u in units:
        out = dot3(u["step"], beside(diagonal(u["step"]), diagonal(u["inv8"])))
        u["step2"] = out[:, :PAIR]
        u["inv"] = u.pop("inv8") - out[:, PAIR:]
        u.pop("step")
    for u in units:
        out = dot3(u["step2"], beside(diagonal(u["step2"]), diagonal(u["inv"])))
        u["step4"] = out[:, :PAIR]
        u["inv"] = u["inv"] + out[:, PAIR:]
        u.pop("step2")
    for u in units:
        u["inv"] = u["inv"] + dot3(u.pop("step4"), diagonal(u["inv"]))
    for u in units:
        right = beside(diagonal(u["value_part"][:CHUNK]), diagonal(u["qu"] * u["half"]))
        u["removed"] = -dot1(u.pop("inv"), right)
    for u in units:
        kept = jnp.concatenate([u["se"] * u["half"], u["sk"] * u["half"]], axis=0)
        right = jnp.concatenate(
            [u["removed"], beside(u["v"], jnp.zeros_like(u["v"]))], axis=0
        )
        out = dot1(kept.T, right)
        u["base"] = undiagonal(out[:, :PAIR])
        u["trans"] = undiagonal(out[:, PAIR:]) + eye * (u["half"] * u["half"])
    return units


def local_reads(units):
    for u in units:
        removed = u["removed"]
        right = beside(diagonal(removed[:, :PAIR]), diagonal(removed[:, PAIR:]))
        out = dot1(u["read_erase"], right)
        u["local"] = out[:, :PAIR] + u["value_part"][CHUNK:]
        u["carried"] = out[:, PAIR:] + u["qr"] * u["half"]


def layer_kernel(
    tokens_hbm, gain_hbm, decay_hbm, key_hbm, rate_hbm, receptance_hbm, value_hbm,
    key_gain_hbm, bias_hbm, shift_hbm, extra_hbm,
    conv_value_hbm, conv_gate_hbm, gate_hbm, taps_hbm, group_gain_hbm, group_shift_hbm,
    head_gain_hbm, conv_out_hbm, mix_out_hbm,
    out_ref,
    gain_ref, key_gain_ref, bias_ref, taps_ref, group_gain_ref, group_shift_ref, head_gain_ref,
    tokens, normed, weights, shift, extra, gate_w, conv_out_w, mix_out_w,
    totals, peer_total, pair_states, y_slots, z_slots, y_seen, z_seen, extended, halo, conv_rows,
    local_rows, carried_rows, gate_gain, conv_full, mix_sent, mix_full, acc,
    sems, load_sems, pair_send, pair_recv, y_send, y_recv, z_send, z_recv, halo_send, halo_recv,
    conv_send, conv_recv, mix_send, mix_recv, small_sems,
):
    sp, tp = lax.axis_index("sp"), lax.axis_index("tp")
    core = lax.rem(sp, 2)
    y = lax.rem(sp // 2, 4)
    z = sp // 8
    sibling = sp + 1 - 2 * core
    after, before = lax.rem(sp + 1, 32), lax.rem(sp + 31, 32)
    is_first = core == 0

    def y_of(step):
        return lax.rem(y + step, 4)

    def z_of(step):
        return lax.rem(z + step, 4)

    def x_of(step):
        return lax.rem(tp + step, 4)

    def y_peer(step):
        return (z * 8 + y_of(step) * 2 + core, tp)

    def z_peer(step):
        return (z_of(step) * 8 + y * 2 + core, tp)

    def x_peer(step):
        return (sp, x_of(step))

    def remote(source, target, send, recv, peer):
        return pltpu.make_async_remote_copy(
            src_ref=source, dst_ref=target, send_sem=send, recv_sem=recv,
            device_id=peer, device_id_type=MESH,
        )

    order = (decay_hbm, key_hbm, rate_hbm, receptance_hbm, value_hbm)
    copies = [pltpu.make_async_copy(tokens_hbm, tokens, sems.at[0])]
    for i, source in enumerate(order):
        copies.append(pltpu.make_async_copy(source, weights.at[i], sems.at[1 + i]))
    copies.append(
        pltpu.make_async_copy(conv_value_hbm, weights.at[5, :, pl.ds(0, PAIR)], sems.at[6])
    )
    late = [
        pltpu.make_async_copy(conv_gate_hbm, weights.at[5, :, pl.ds(PAIR, PAIR)], sems.at[7]),
        pltpu.make_async_copy(shift_hbm, shift, sems.at[8]),
        pltpu.make_async_copy(extra_hbm, extra, sems.at[9]),
    ]
    smalls = [
        pltpu.make_async_copy(source, target, small_sems.at[i])
        for i, (source, target) in enumerate(
            (
                (gain_hbm, gain_ref),
                (key_gain_hbm, key_gain_ref),
                (bias_hbm, bias_ref),
                (taps_hbm, taps_ref),
                (group_gain_hbm, group_gain_ref),
                (group_shift_hbm, group_shift_ref),
                (head_gain_hbm, head_gain_ref),
            )
        )
    ]
    copies[0].start()
    smalls[0].start()
    for copy in copies[1:] + late:
        copy.start()
    for copy in smalls[1:]:
        copy.start()

    barrier = pltpu.get_barrier_semaphore()
    peers = [(sibling, tp), (after, tp), (before, tp)]
    for step in (1, 2, 3):
        peers += [y_peer(step), z_peer(step), x_peer(step)]
    for peer in peers:
        pl.semaphore_signal(barrier, inc=1, device_id=peer, device_id_type=MESH)

    loads = [
        pltpu.make_async_copy(gate_hbm, gate_w, load_sems.at[0]),
        pltpu.make_async_copy(conv_out_hbm, conv_out_w, load_sems.at[1]),
        pltpu.make_async_copy(mix_out_hbm, mix_out_w, load_sems.at[2]),
    ]
    eye = (iota((HEAD, 2 * PAIR), 0) == iota((HEAD, 2 * PAIR), 1) % HEAD) & (
        iota((HEAD, 2 * PAIR), 1) < PAIR
    )
    identity = jnp.where(eye, 1.0, 0.0).astype(BF16)
    for k in range(3):
        y_seen[k] = identity
        z_seen[k] = identity
    with jax.named_scope("wait_tokens"):
        copies[0].wait()
        smalls[0].wait()
    with jax.named_scope("norm"):
        normed[...] = normalize(tokens[...], gain_ref[...])
    with jax.named_scope("project"):
        found = []
        for i in (0, 2, 4):
            copies[1 + i].wait()
            copies[2 + i].wait()
            if i == 4:
                late[0].wait()
            found.append(dot(normed[...], weights[i]))
            found.append(dot(normed[...], weights[i + 1]))
        decay, key, rate, receptance, value, conv_both = (rounded(rows) for rows in found)
        for copy in late[1:] + smalls[1:]:
            copy.wait()
    for load in loads:
        load.start()
    with jax.named_scope("algebra"):
        units = chunk_algebra(
            receptance, key, value, decay, rate, key_gain_ref[...], bias_ref[...], shift[...],
            extra[...],
        )
    with jax.named_scope("totals"):
        prefixes = []
        for p in range(2):
            steps = [(u["trans"], u["base"]) for u in units if u["p"] == p]
            two = compose(steps[1], steps[0], dot3)
            upper = compose(steps[3], steps[2], dot3)
            totals[p] = beside(*compose(upper, two, dot3))
            prefixes.append((steps[0], two, steps[2]))
    with jax.named_scope("barrier"):
        pl.semaphore_wait(barrier, len(peers))
    pair_copy = remote(
        totals.at[1 - core], peer_total, pair_send.at[0], pair_recv.at[0], (sibling, tp)
    )
    pair_copy.start()

    with jax.named_scope("conv_project"):
        conv_input = (conv_both[:, :PAIR] * sigmoid(conv_both[:, PAIR:])).astype(BF16)
        conv_rows[...] = conv_input[224:]
        halo_copy = remote(conv_rows, halo, halo_send.at[0], halo_recv.at[0], (after, tp))
        pl.when(sp < 31)(halo_copy.start)
        extended[:32, :] = jnp.zeros((32, PAIR), F32)
        extended[32:, :] = conv_input.astype(F32)

    with jax.named_scope("pair_wait"):
        pair_copy.wait()
    with jax.named_scope("pair_compose"):
        own, other = totals[core], peer_total[...]
        first = jnp.where(is_first, own, other)
        second = jnp.where(is_first, other, own)
        chip_first = (first[:, :PAIR], first[:, PAIR:])
        chip = compose((second[:, :PAIR], second[:, PAIR:]), chip_first, dot3)
        y_slots[y] = beside(*chip).astype(BF16)
    y_copies = []
    for step in (2, 1, 3):
        copy = remote(
            y_slots.at[y], y_slots.at[y], y_send.at[step - 1], y_recv.at[step - 1], y_peer(step)
        )
        copy.start()
        y_copies.append(copy)

    with jax.named_scope("gate_project"):
        loads[0].wait()
        gated = sigmoid(rounded(dot(normed[...], gate_w[...]))) * head_gain_ref[...]
        gate_gain[0] = gated[:, :PAIR]
        gate_gain[1] = gated[:, PAIR:]
    with jax.named_scope("local_reads"):
        local_reads(units)
        for p in range(2):
            one, two, third = prefixes[p]
            earlier = (None, one, two, compose(third, two, dot1))
            for u in units:
                if u["p"] != p:
                    continue
                c = u["c"]
                rows = slice(c * CHUNK, (c + 1) * CHUNK)
                if c == 0:
                    local_rows[p, rows] = u["local"]
                    carried_rows[p, rows] = u["carried"]
                    continue
                right = beside(diagonal(earlier[c][0]), diagonal(earlier[c][1]))
                out = dot1(u["carried"], right)
                carried_rows[p, rows] = out[:, :PAIR]
                local_rows[p, rows] = out[:, PAIR:] + u["local"]

    def y_arrival(step):
        arrived = y_of(4 - step)
        return remote(
            y_slots.at[arrived], y_slots.at[arrived], y_send.at[step - 1], y_recv.at[step - 1],
            y_peer(step),
        )

    with jax.named_scope("y_wait_lower"):
        for step in (1, 2, 3):

            @pl.when(step <= y)
            def _(step=step):
                y_arrival(step).wait_recv()
                y_seen[y - step] = y_slots[y - step]

    def slot(ref, k):
        both = ref[k].astype(F32)
        return both[:, :PAIR], both[:, PAIR:]

    with jax.named_scope("before_chip"):
        before_chip = compose(
            slot(y_seen, 2), compose(slot(y_seen, 1), slot(y_seen, 0), dot1), dot3
        )
        before_second = compose(chip_first, before_chip, dot3)
        trans_both = jnp.concatenate([before_chip[0], before_second[0]], axis=0)
        base_both = jnp.concatenate([before_chip[1], before_second[1]], axis=0)

    with jax.named_scope("halo_wait"):

        @pl.when(sp > 0)
        def _():
            halo_copy.wait_recv()
            extended[:32, :] = halo[...].astype(F32)

    with jax.named_scope("convolution"):
        taps = taps_ref[...]
        conv_sum = jnp.zeros((256, PAIR), F32)
        for j in range(31):
            conv_sum = conv_sum + taps[j : j + 1] * extended[pl.ds(2 + j, 256), :]
        normal = group_norm(conv_sum, group_ones(PAIR), GROUP_EPS)
        affine = normal * group_gain_ref[...] + group_shift_ref[...]
        conv_out = (affine * sigmoid(affine)).astype(BF16)
        for k in range(4):
            conv_full[0, k] = conv_out[k * 64 : (k + 1) * 64]
    conv_copies = []
    for step in (2, 1, 3):
        copy = remote(
            conv_full.at[0, x_of(step)], conv_full.at[1, tp],
            conv_send.at[step - 1], conv_recv.at[step - 1], x_peer(step),
        )
        copy.start()
        conv_copies.append(copy)

    with jax.named_scope("y_wait_upper"):
        for step in (1, 2, 3):
            pl.when(step > y)(y_arrival(step).wait_recv)

    def z_copy(step):
        return remote(
            z_slots.at[z], z_slots.at[z], z_send.at[step - 1], z_recv.at[step - 1], z_peer(step)
        )

    with jax.named_scope("plane"):

        @pl.when(z < 3)
        def _():
            lower = compose(slot(y_slots, 1), slot(y_slots, 0), dot1)
            upper = compose(slot(y_slots, 3), slot(y_slots, 2), dot1)
            z_slots[z] = beside(*compose(upper, lower, dot3)).astype(BF16)
            z_copy(1).start()
            pl.when(z < 2)(z_copy(2).start)
            pl.when(z < 1)(z_copy(3).start)

    with jax.named_scope("z_wait"):
        for step in (1, 3, 2):

            @pl.when(step <= z)
            def _(step=step):
                below = z - step
                remote(
                    z_slots.at[below], z_slots.at[below], z_send.at[step - 1],
                    z_recv.at[step - 1], z_peer(step),
                ).wait_recv()
                z_seen[below] = z_slots[below]

    with jax.named_scope("z_compose"):
        p0, p1, p2 = (slot(z_seen, k) for k in range(3))
        inner = dot1(p1[0], diagonal(p0[1])) + p1[1]
        out = dot3(trans_both, beside(diagonal(p2[0]), diagonal(p2[1])))
        states = dot3(out[:, :PAIR], diagonal(inner)) + (out[:, PAIR:] + base_both)
        state_first, state_second = states[:HEAD], states[HEAD:]
        mine = jnp.where(is_first, state_first, state_second)
        pair_states[0] = jnp.where(is_first, state_second, state_first)
    state_copy = remote(
        pair_states.at[0], pair_states.at[1], pair_send.at[1], pair_recv.at[1], (sibling, tp)
    )
    state_copy.start()

    ones = group_ones(PAIR)

    def read_pair(p, state, half):
        readout = local_rows[p] + dot3(carried_rows[p], diagonal(state))
        mix_out = (group_norm(readout, ones, HEAD_EPS) * gate_gain[p]).astype(BF16)
        started = []
        for k in range(4):
            mix_sent[half, k] = mix_out[k * 64 : (k + 1) * 64]
        for step in (2, 1, 3):
            copy = remote(
                mix_sent.at[half, x_of(step)], mix_full.at[half, tp],
                mix_send.at[half, step - 1], mix_recv.at[half, step - 1], x_peer(step),
            )
            copy.start()
            started.append(copy)
        return started

    def out_rows(owner, p):
        return pl.ds(pl.multiple_of(owner * 256 + p * PAIR, PAIR), PAIR)

    with jax.named_scope("read_own"):
        started = read_pair(core, mine, 0)

    with jax.named_scope("conv_project_out"):
        loads[1].wait()
        acc[...] = dot(conv_full[0, tp], conv_out_w[pl.ds(pl.multiple_of(tp * PAIR, PAIR), PAIR), :])
        for step in (1, 3, 2):
            arrived = x_of(4 - step)
            remote(
                conv_full.at[0, arrived], conv_full.at[1, arrived],
                conv_send.at[step - 1], conv_recv.at[step - 1], x_peer(step),
            ).wait_recv()
            rows = pl.ds(pl.multiple_of(arrived * PAIR, PAIR), PAIR)
            acc[...] += dot(conv_full[1, arrived], conv_out_w[rows, :])
    with jax.named_scope("state_wait"):
        state_copy.wait()
    with jax.named_scope("read_other"):
        started += read_pair(1 - core, pair_states[1], 1)
    with jax.named_scope("mix_own"):
        loads[2].wait()
        acc[...] += dot(mix_sent[0, tp], mix_out_w[out_rows(tp, core), :]) + dot(
            mix_sent[1, tp], mix_out_w[out_rows(tp, 1 - core), :]
        )
    for half in (0, 1):
        for step in (1, 3, 2):
            arrived = x_of(4 - step)
            with jax.named_scope("mix_wait"):
                remote(
                    mix_sent.at[half, arrived], mix_full.at[half, arrived],
                    mix_send.at[half, step - 1], mix_recv.at[half, step - 1], x_peer(step),
                ).wait_recv()
            with jax.named_scope("mix_project"):
                p = core if half == 0 else 1 - core
                acc[...] += dot(mix_full[half, arrived], mix_out_w[out_rows(arrived, p), :])
    out_ref[...] = acc[...].astype(BF16)
    for copy in y_copies + conv_copies + started:
        copy.wait_send()
    pl.when(sp < 31)(halo_copy.wait_send)
    for step in (1, 2, 3):
        pl.when(z + step < 4)(z_copy(step).wait_send)


VMEM = pl.BlockSpec(memory_space=pltpu.VMEM)
ANY = pl.BlockSpec(memory_space=pltpu.HBM)


def local(
    tokens, input_norm_gain, convolution_value_weight, convolution_gate_weight,
    depthwise_taps_weight, convolution_group_gain, convolution_group_shift, receptance_weight,
    key_weight, value_weight, decay_weight, correction_rate_weight, output_gate_weight,
    key_prenorm_gain, decay_offset_bias, position_decay_shift, extra_log_decay, head_norm_gain,
    convolution_output_weight, attention_output_weight,
):
    dma = pltpu.SemaphoreType.DMA
    return pl.pallas_call(
        layer_kernel,
        name="layer",
        out_shape=pltpu.VMEM((64, 2048), BF16),
        in_specs=[ANY] * 20,
        out_specs=VMEM,
        scratch_shapes=[
            pltpu.VMEM((1, 2048), F32),
            pltpu.VMEM((1, 256), F32),
            pltpu.VMEM((1, 256), F32),
            pltpu.VMEM((31, 128), F32),
            pltpu.VMEM((1, 128), F32),
            pltpu.VMEM((1, 128), F32),
            pltpu.VMEM((1, 256), F32),
            pltpu.VMEM((256, 2048), BF16),
            pltpu.VMEM((256, 2048), BF16),
            pltpu.VMEM((6, 2048, 256), BF16),
            pltpu.VMEM((256, 256), F32),
            pltpu.VMEM((256, 256), F32),
            pltpu.VMEM((2048, 256), BF16),
            pltpu.VMEM((512, 2048), BF16),
            pltpu.VMEM((1024, 2048), BF16),
            pltpu.VMEM((2, 64, 256), F32),
            pltpu.VMEM((64, 256), F32),
            pltpu.VMEM((2, 64, 128), F32),
            pltpu.VMEM((4, 64, 256), BF16),
            pltpu.VMEM((4, 64, 256), BF16),
            pltpu.VMEM((3, 64, 256), BF16),
            pltpu.VMEM((3, 64, 256), BF16),
            pltpu.VMEM((288, 128), F32),
            pltpu.VMEM((32, 128), BF16),
            pltpu.VMEM((32, 128), BF16),
            pltpu.VMEM((2, 256, 128), F32),
            pltpu.VMEM((2, 256, 128), F32),
            pltpu.VMEM((2, 256, 128), F32),
            pltpu.VMEM((2, 4, 64, 128), BF16),
            pltpu.VMEM((2, 4, 64, 128), BF16),
            pltpu.VMEM((2, 4, 64, 128), BF16),
            pltpu.VMEM((64, 2048), F32),
            dma((10,)), dma((3,)), dma((2,)), dma((2,)), dma((3,)), dma((3,)), dma((3,)), dma((3,)),
            dma((1,)), dma((1,)), dma((3,)), dma((3,)), dma((2, 3)), dma((2, 3)), dma((7,)),
        ],
        compiler_params=pltpu.CompilerParams(
            collective_id=0, has_side_effects=True, vmem_limit_bytes=56000000
        ),
    )(
        *(
            pltpu.with_memory_space_constraint(operand, pltpu.HBM)
            for operand in (
                tokens, input_norm_gain.reshape(1, -1), decay_weight, key_weight,
                correction_rate_weight, receptance_weight, value_weight,
                key_prenorm_gain.reshape(1, -1), decay_offset_bias.reshape(1, -1),
                position_decay_shift, extra_log_decay, convolution_value_weight,
                convolution_gate_weight, output_gate_weight, depthwise_taps_weight,
                convolution_group_gain.reshape(1, -1), convolution_group_shift.reshape(1, -1),
                head_norm_gain.reshape(1, -1), convolution_output_weight, attention_output_weight,
            )
        )
    )


def solution(mesh):
    rows, chans, vec = P("sp", None), P(None, "tp"), P("tp")
    placed = (
        rows, P(), chans, chans, chans, vec, vec, chans, chans, chans, chans, chans, chans,
        vec, vec, P("sp", "tp"), P("sp", "tp"), vec, P(), P(),
    )
    return jax.shard_map(
        local, mesh=mesh, in_specs=placed, out_specs=P(("sp", "tp"), None), check_vma=False
    )
```

```python
import functools

import jax
import jax.numpy as jnp
from jax import lax
from jax.experimental import pallas as pl
from jax.experimental.pallas import tpu as pltpu
from jax.sharding import PartitionSpec as P

F32 = jnp.float32
BF16 = jnp.bfloat16
MESH = pl.DeviceIdType.MESH
HEAD = 64
CHUNK = 64
PAIR = 128

NORM_EPS = 1e-06
GROUP_EPS = 1e-05
HEAD_EPS = 0.00064
KEY_EPS = 1e-06

NN = (((1,), (0,)), ((), ()))
NT = (((1,), (1,)), ((), ()))


def dot(left, right, dims=NN):
    return lax.dot_general(left, right, dims, preferred_element_type=F32)


def split(values):
    high = values.astype(BF16)
    return high, (values - high.astype(F32)).astype(BF16)


def dot1(left, right, dims=NN):
    return dot(left.astype(BF16), right.astype(BF16), dims)


def dot3(left, right, dims=NN):
    left_high, left_low = split(left)
    right_high, right_low = split(right)
    return dot(left_high, right_high, dims) + (
        dot(left_low, right_high, dims) + dot(left_high, right_low, dims)
    )


def dot2(left, right_exact):
    high, low = split(left)
    return dot(high, right_exact) + dot(low, right_exact)


def iota(shape, dim):
    return lax.broadcasted_iota(jnp.int32, shape, dim)


def first_head(rows):
    return iota((rows, PAIR), 1) < HEAD


def diagonal(packed):
    mask = first_head(packed.shape[0])
    return jnp.concatenate([jnp.where(mask, packed, 0.0), jnp.where(mask, 0.0, packed)], axis=0)


def undiagonal(full):
    return jnp.where(first_head(HEAD), full[:HEAD], full[HEAD:])


def beside(*parts):
    return jnp.concatenate(parts, axis=1)


def group_ones(width):
    return (iota((width, width), 0) // HEAD == iota((width, width), 1) // HEAD).astype(BF16)


def sigmoid(values):
    return 1.0 / (1.0 + jnp.exp(-values))


def rounded(values):
    return values.astype(BF16).astype(F32)


def normalize(tokens, gain):
    rows = tokens.astype(F32)
    scale = lax.rsqrt(jnp.mean(rows * rows, axis=-1, keepdims=True) + NORM_EPS)
    return (rows * scale * gain).astype(BF16)


def group_norm(values, ones, eps):
    centred = values - dot2(values, ones) * (1.0 / HEAD)
    return centred * lax.rsqrt(dot2(centred * centred, ones) * (1.0 / HEAD) + eps)


def compose(later, earlier, product):
    trans, base = later
    out = product(trans, beside(diagonal(earlier[0]), diagonal(earlier[1])))
    return out[:, :PAIR], out[:, PAIR:] + base


def chunk_algebra(receptance, key, value, decay, rate, key_gain, decay_bias, shift, extra):
    tok_rows, width = receptance.shape
    chunks, pairs = tok_rows // CHUNK, width // PAIR
    logits = decay + decay_bias + shift
    log_decay = sigmoid(logits) * (-0.6065306597126334) + extra
    scaled = key * key_gain
    ones = group_ones(width)
    unit = scaled * lax.rsqrt(dot2(scaled * scaled, ones) + KEY_EPS)
    erase = unit * sigmoid(rate)
    value = value - dot(value.astype(BF16), ones) * (1.0 / HEAD)
    row, col = iota((tok_rows, tok_rows), 0), iota((tok_rows, tok_rows), 1)
    running = ((row // CHUNK == col // CHUNK) & (row >= col)).astype(BF16)
    high, low = split(log_decay)
    total = dot(running, high) + dot(running, low)

    strict_rows = iota((CHUNK, PAIR), 0)
    strict_cols = iota((CHUNK, PAIR), 1) % HEAD
    strict = strict_rows > strict_cols
    inclusive = strict_rows >= strict_cols
    eye = (strict_rows == strict_cols).astype(F32)
    same8 = (strict_rows // 8) == (strict_cols // 8)
    lane_first = first_head(CHUNK)

    units = []
    for c in range(chunks):
        rows = slice(c * CHUNK, (c + 1) * CHUNK)
        cum = total[rows]
        last = cum[CHUNK - 1 : CHUNK]
        half = 0.5 * last
        grow = jnp.exp(half - cum)
        shrink = jnp.exp(cum - half)
        half_decay = jnp.exp(half)
        query_unit = unit[rows] * jnp.exp(cum - log_decay[rows] - half)
        query_read = receptance[rows] * shrink
        scaled_erase = erase[rows] * grow
        scaled_key = key[rows] * grow
        for p in range(pairs):
            lanes = slice(p * PAIR, (p + 1) * PAIR)
            units.append(
                dict(
                    c=c,
                    p=p,
                    qu=query_unit[:, lanes],
                    qr=query_read[:, lanes],
                    se=scaled_erase[:, lanes],
                    sk=scaled_key[:, lanes],
                    v=value[rows, lanes],
                    half=half_decay[:, lanes],
                )
            )
    for u in units:
        left = jnp.concatenate([u["qu"], u["qr"]], axis=0)
        right = jnp.concatenate([diagonal(u["se"]), diagonal(u["sk"])], axis=0)
        u["gram"] = dot1(left, right, NT)
    for u in units:
        gram = u.pop("gram")
        u["mix"] = jnp.where(strict, gram[:CHUNK, :PAIR], 0.0)
        u["key_mix"] = jnp.where(strict, gram[:CHUNK, PAIR:], 0.0)
        u["read_erase"] = jnp.where(inclusive, gram[CHUNK:, :PAIR], 0.0)
        u["read_key"] = jnp.where(inclusive, gram[CHUNK:, PAIR:], 0.0)
        u["near"] = jnp.where(same8, u["mix"], 0.0)
        u["far"] = jnp.where(same8, 0.0, u["mix"])
    for u in units:
        u["near2"] = dot3(u["near"], diagonal(u["near"]))
        u["value_part"] = dot1(
            jnp.concatenate([u.pop("key_mix"), u.pop("read_key")], axis=0), diagonal(u["v"])
        )
    for u in units:
        powers = dot3(jnp.concatenate([u["near"], u["near2"]], axis=0), diagonal(u["near2"]))
        u["start"] = eye - u.pop("near") + u.pop("near2") - powers[:CHUNK]
        u["near4"] = powers[CHUNK:]
    for u in units:
        u["inv8"] = u["start"] + dot3(u["start"], diagonal(u.pop("near4")))
        u.pop("start")
    for u in units:
        right = beside(
            diagonal(u.pop("far")), diagonal(u["value_part"][:CHUNK]), diagonal(u["qu"] * u["half"])
        )
        out = dot1(u.pop("inv8"), right)
        u["step"], u["removed"] = out[:, :PAIR], -out[:, PAIR:]
    for sign, last in ((-1.0, False), (1.0, False), (1.0, True)):
        for u in units:
            step, removed = u.pop("step"), u["removed"]
            parts = [diagonal(removed[:, :PAIR]), diagonal(removed[:, PAIR:])]
            if not last:
                parts.append(diagonal(step))
            out = dot1(step, beside(*parts))
            u["removed"] = removed + sign * out[:, : 2 * PAIR]
            if not last:
                u["step"] = out[:, 2 * PAIR :]
    for u in units:
        kept = jnp.concatenate([u["se"] * u["half"], u["sk"] * u["half"]], axis=0)
        right = jnp.concatenate(
            [u["removed"], beside(u["v"], jnp.zeros_like(u["v"]))], axis=0
        )
        out = dot1(kept.T, right)
        u["base"] = undiagonal(out[:, :PAIR])
        u["trans"] = undiagonal(out[:, PAIR:]) + eye * (u["half"] * u["half"])
    return units


def local_reads(units):
    for u in units:
        removed = u["removed"]
        right = beside(diagonal(removed[:, :PAIR]), diagonal(removed[:, PAIR:]))
        out = dot1(u["read_erase"], right)
        u["local"] = out[:, :PAIR] + u["value_part"][CHUNK:]
        u["carried"] = out[:, PAIR:] + u["qr"] * u["half"]


def layer_kernel(
    tokens_hbm, gain_hbm, decay_hbm, key_hbm, rate_hbm, receptance_hbm, value_hbm,
    key_gain_hbm, bias_hbm, shift_hbm, extra_hbm,
    conv_value_hbm, conv_gate_hbm, gate_hbm, taps_hbm, group_gain_hbm, group_shift_hbm,
    head_gain_hbm, conv_out_hbm, mix_out_hbm,
    out_ref,
    gain_ref, key_gain_ref, bias_ref, taps_ref, group_gain_ref, group_shift_ref, head_gain_ref,
    tokens, normed, weights, shift, extra, gate_w, conv_out_w, mix_out_w,
    totals, peer_total, pair_states, y_slots, z_slots, y_seen, z_seen, raw_slots, raw_seen, extended, halo, conv_rows,
    local_rows, carried_rows, gate_gain, conv_full, mix_sent, mix_full, acc,
    sems, load_sems, pair_send, pair_recv, y_send, y_recv, z_send, z_recv, halo_send, halo_recv,
    conv_send, conv_recv, mix_send, mix_recv, small_sems, raw_send, raw_recv,
):
    sp, tp = lax.axis_index("sp"), lax.axis_index("tp")
    core = lax.rem(sp, 2)
    y = lax.rem(sp // 2, 4)
    z = sp // 8
    sibling = sp + 1 - 2 * core
    after = lax.rem(sp + 1, 32)
    is_first = core == 0

    def y_source(step):
        return z * 8 + lax.rem(y + 4 - step, 4) * 2 + core

    def y_target(step):
        return z * 8 + lax.rem(y + step, 4) * 2 + core

    def x_of(step):
        return lax.rem(tp + step, 4)

    def x_peer(step):
        return (sp, x_of(step))

    def remote(source, target, send, recv, peer):
        return pltpu.make_async_remote_copy(
            src_ref=source, dst_ref=target, send_sem=send, recv_sem=recv,
            device_id=peer, device_id_type=MESH,
        )

    order = (decay_hbm, key_hbm, rate_hbm, receptance_hbm, value_hbm)
    copies = [pltpu.make_async_copy(tokens_hbm, tokens, sems.at[0])]
    for i, source in enumerate(order):
        copies.append(pltpu.make_async_copy(source, weights.at[i], sems.at[1 + i]))
    late = [
        pltpu.make_async_copy(shift_hbm, shift, sems.at[6]),
        pltpu.make_async_copy(extra_hbm, extra, sems.at[7]),
    ]
    smalls = [
        pltpu.make_async_copy(source, target, small_sems.at[i])
        for i, (source, target) in enumerate(
            (
                (gain_hbm, gain_ref),
                (key_gain_hbm, key_gain_ref),
                (bias_hbm, bias_ref),
                (taps_hbm, taps_ref),
                (group_gain_hbm, group_gain_ref),
                (group_shift_hbm, group_shift_ref),
                (head_gain_hbm, head_gain_ref),
            )
        )
    ]
    copies[0].start()
    smalls[0].start()
    for copy in copies[1:] + late:
        copy.start()
    for copy in smalls[1:]:
        copy.start()

    barrier = pltpu.get_barrier_semaphore()

    def greet(peer):
        pl.semaphore_signal(barrier, inc=1, device_id=peer, device_id_type=MESH)

    greet((sibling, tp))
    pl.when(sp > 0)(lambda: greet((sp - 1, tp)))
    for step in (1, 2, 3):
        meets = (step <= y) | ((z < 3) & (y > 0)) if step == 1 else (step <= y) | (z < 3)
        pl.when(meets)(lambda step=step: greet((y_source(step), tp)))
        pl.when((y == 0) & (step <= z))(
            lambda step=step: greet(((z - step) * 8 + 6 + core, tp))
        )
        pl.when(step <= z)(lambda step=step: greet((sp - 8 * step, tp)))
        greet(x_peer(step))
    targets = (
        4 + jnp.where(sp < 31, 1, 0) + jnp.where(z < 3, jnp.where(y == 3, 2, 3), 3 - y) + (3 - z)
        + jnp.where(y == 3, 3 - z, 0)
    )

    loads = [
        pltpu.make_async_copy(gate_hbm, gate_w, load_sems.at[0]),
        pltpu.make_async_copy(conv_value_hbm, weights.at[5, :, pl.ds(0, PAIR)], load_sems.at[3]),
        pltpu.make_async_copy(
            conv_gate_hbm, weights.at[5, :, pl.ds(PAIR, PAIR)], load_sems.at[4]
        ),
        pltpu.make_async_copy(conv_out_hbm, conv_out_w, load_sems.at[1]),
        pltpu.make_async_copy(mix_out_hbm, mix_out_w, load_sems.at[2]),
    ]
    eye = (iota((HEAD, 2 * PAIR), 0) == iota((HEAD, 2 * PAIR), 1) % HEAD) & (
        iota((HEAD, 2 * PAIR), 1) < PAIR
    )
    identity = jnp.where(eye, 1.0, 0.0).astype(BF16)
    for k in range(3):
        y_seen[k] = identity
        raw_seen[k] = identity
        z_seen[k, 0] = identity[:, :PAIR]
        z_seen[k, 1] = identity[:, PAIR:]
    with jax.named_scope("wait_tokens"):
        copies[0].wait()
        smalls[0].wait()
    with jax.named_scope("norm"):
        normed[...] = normalize(tokens[...], gain_ref[...])
    with jax.named_scope("project"):
        found = []
        for i in (0, 2):
            copies[1 + i].wait()
            copies[2 + i].wait()
            found.append(dot(normed[...], weights[i]))
            found.append(dot(normed[...], weights[i + 1]))
        copies[5].wait()
        half = weights.shape[1] // 2
        keep = jnp.where(sp < 32, 1.0, 0.0)
        found.append(
            dot(normed[:, :half], weights[4, :half, :])
            + keep * dot(normed[:, half:], weights[4, half:, :])
        )
        decay, key, rate, receptance, value = (rounded(rows) for rows in found)
        for copy in late + smalls[1:]:
            copy.wait()
    for load in loads:
        load.start()
    with jax.named_scope("algebra"):
        units = chunk_algebra(
            receptance, key, value, decay, rate, key_gain_ref[...], bias_ref[...], shift[...],
            extra[...],
        )
    with jax.named_scope("totals"):
        prefixes = []
        for p in range(2):
            steps = [(u["trans"], u["base"]) for u in units if u["p"] == p]
            two = compose(steps[1], steps[0], dot3)
            upper = compose(steps[3], steps[2], dot3)
            totals[p] = beside(*compose(upper, two, dot3))
            prefixes.append((steps[0], two, steps[2]))
    with jax.named_scope("barrier"):
        pl.semaphore_wait(barrier, targets)
    pair_copy = remote(
        totals.at[1 - core], peer_total, pair_send.at[0], pair_recv.at[0], (sibling, tp)
    )
    pair_copy.start()

    with jax.named_scope("conv_project"):
        for load in loads[:3]:
            load.wait()
        gate_rows = dot(normed[...], gate_w[...])
        conv_both = rounded(dot(normed[...], weights[5]))
        conv_input = (conv_both[:, :PAIR] * sigmoid(conv_both[:, PAIR:])).astype(BF16)
        conv_rows[...] = conv_input[224:]
        halo_copy = remote(conv_rows, halo, halo_send.at[0], halo_recv.at[0], (after, tp))
        pl.when(sp < 31)(halo_copy.start)
        extended[:32, :] = jnp.zeros((32, PAIR), F32)
        extended[32:, :] = conv_input.astype(F32)

    with jax.named_scope("gate_project"):
        gated = sigmoid(rounded(gate_rows)) * head_gain_ref[...]
        gate_gain[0] = gated[:, :PAIR]
        gate_gain[1] = gated[:, PAIR:]
    with jax.named_scope("pair_wait"):
        pair_copy.wait()
    with jax.named_scope("pair_compose"):
        own, other = totals[core], peer_total[...]
        first = jnp.where(is_first, own, other)
        second = jnp.where(is_first, other, own)
        chip_first = (first[:, :PAIR], first[:, PAIR:])
        chip = compose((second[:, :PAIR], second[:, PAIR:]), chip_first, dot3)
        y_slots[y] = beside(*chip).astype(BF16)

    def y_copy(step, slot, peer):
        return remote(
            y_slots.at[slot], y_slots.at[slot], y_send.at[step - 1], y_recv.at[step - 1],
            (peer, tp),
        )

    def raw_copy(up, slot, plane, peer):
        return remote(
            y_slots.at[slot], raw_slots.at[plane], raw_send.at[up - 1], raw_recv.at[plane],
            (peer, tp),
        )

    def raw_target(up):
        return (z + up) * 8 + core

    for up in (1, 2, 3):
        pl.when((y == 3) & (z + up < 4))(
            lambda up=up: raw_copy(up, y, z, raw_target(up)).start()
        )

    def y_sends(step):
        return (y + step < 4) | ((z < 3) & (y < 3)) if step == 1 else (y + step < 4) | (z < 3)

    for step in (2, 3, 1):
        pl.when(y_sends(step))(lambda step=step: y_copy(step, y, y_target(step)).start())

    with jax.named_scope("local_reads"):
        local_reads(units)
        for p in range(2):
            one, two, third = prefixes[p]
            earlier = (None, one, two, compose(third, two, dot1))
            for u in units:
                if u["p"] != p:
                    continue
                c = u["c"]
                rows = slice(c * CHUNK, (c + 1) * CHUNK)
                if c == 0:
                    local_rows[p, rows] = u["local"]
                    carried_rows[p, rows] = u["carried"]
                    continue
                right = beside(diagonal(earlier[c][0]), diagonal(earlier[c][1]))
                out = dot1(u["carried"], right)
                carried_rows[p, rows] = out[:, :PAIR]
                local_rows[p, rows] = out[:, PAIR:] + u["local"]

    with jax.named_scope("y_wait_lower"):
        for step in (1, 2, 3):

            @pl.when(step <= y)
            def _(step=step):
                y_copy(step, y - step, sibling).wait_recv()
                y_seen[y - step] = y_slots[y - step]

    def slot(ref, k):
        both = ref[k].astype(F32)
        return both[:, :PAIR], both[:, PAIR:]

    with jax.named_scope("before_chip"):
        before_chip = compose(
            slot(y_seen, 2), compose(slot(y_seen, 1), slot(y_seen, 0), dot1), dot3
        )
        before_second = compose(chip_first, before_chip, dot3)
        trans_both = jnp.concatenate([before_chip[0], before_second[0]], axis=0)
        base_both = jnp.concatenate([before_chip[1], before_second[1]], axis=0)

    with jax.named_scope("halo_wait"):

        @pl.when(sp > 0)
        def _():
            halo_copy.wait_recv()
            extended[:32, :] = halo[...].astype(F32)

    with jax.named_scope("convolution"):
        taps = taps_ref[...]
        conv_sum = jnp.zeros((256, PAIR), F32)
        for j in range(31):
            conv_sum = conv_sum + taps[j : j + 1] * extended[pl.ds(2 + j, 256), :]
        normal = group_norm(conv_sum, group_ones(PAIR), GROUP_EPS)
        affine = normal * group_gain_ref[...] + group_shift_ref[...]
        conv_out = (affine * sigmoid(affine)).astype(BF16)
        for k in range(4):
            conv_full[0, k] = conv_out[k * 64 : (k + 1) * 64]
    conv_copies = []
    for step in (2, 1, 3):
        copy = remote(
            conv_full.at[0, x_of(step)], conv_full.at[1, tp],
            conv_send.at[step - 1], conv_recv.at[step - 1], x_peer(step),
        )
        copy.start()
        conv_copies.append(copy)

    def z_copy(up, kind, slot, peer):
        return remote(
            z_slots.at[slot, kind], z_slots.at[slot, kind], z_send.at[up - 1, kind],
            z_recv.at[slot, kind], (peer, tp),
        )

    def z_column(up):
        z_copy(up, 1, z, sp + 8 * up).start()
        pl.when(z > 0)(z_copy(up, 0, z, sp + 8 * up).start)

    def upper(step):
        y_copy(step, lax.rem(y + 4 - step, 4), sibling).wait_recv()

    with jax.named_scope("plane"):

        @pl.when(z < 3)
        def _():
            for step in (3, 2):
                pl.when(step > y)(lambda step=step: upper(step))
            lower = compose(slot(y_slots, 1), slot(y_slots, 0), dot1)

            def store(total):
                z_slots[z, 0] = total[0].astype(BF16)
                z_slots[z, 1] = total[1].astype(BF16)

            @pl.when(y == 0)
            def _():
                store(compose(slot(y_slots, 2), lower, dot3))

            @pl.when(y > 0)
            def _():
                store(compose(compose(slot(y_slots, 3), slot(y_slots, 2), dot1), lower, dot3))

            z_column(1)
            pl.when(z < 2)(lambda: z_column(2))
            pl.when(z < 1)(lambda: z_column(3))

    def z_arrival(below):
        @pl.when(below > 0)
        def _():
            z_copy(1, 0, below, sibling).wait_recv()

        z_copy(1, 1, below, sibling).wait_recv()

    with jax.named_scope("z_wait"):
        for below in range(2):

            @pl.when(below < z - 1)
            def _(below=below):
                z_arrival(below)
                if below > 0:
                    z_seen[below, 0] = z_slots[below, 0]
                z_seen[below, 1] = z_slots[below, 1]

        for below in range(3):

            @pl.when((y == 0) & (below < z))
            def _(below=below):
                raw_copy(1, 0, below, sibling).wait_recv()
                raw_seen[jnp.where(below < z - 1, below, 2)] = raw_slots[below]

        def through(parts, state):
            return dot3(parts[0], diagonal(state)) + parts[1]

        def plane_below(k):
            return z_seen[k, 0].astype(F32), z_seen[k, 1].astype(F32)

        far = through(slot(raw_seen, 0), z_seen[0, 1].astype(F32))
        far = through(slot(raw_seen, 1), through(plane_below(1), far))
        passed = raw_seen[2]
        out = dot3(
            trans_both,
            beside(
                diagonal(passed[:, :PAIR].astype(F32)), diagonal(passed[:, PAIR:].astype(F32))
            ),
        )
        trans_last, base_last = out[:, :PAIR], out[:, PAIR:] + base_both

        @pl.when(z > 0)
        def _():
            z_arrival(z - 1)

            @pl.when(z > 1)
            def _():
                z_seen[2, 0] = z_slots[z - 1, 0]

            z_seen[2, 1] = z_slots[z - 1, 1]

    with jax.named_scope("z_compose"):
        entering = through(plane_below(2), far)
        states = dot3(trans_last, diagonal(entering)) + base_last
        state_first, state_second = states[:HEAD], states[HEAD:]
        mine = jnp.where(is_first, state_first, state_second)
        pair_states[0] = jnp.where(is_first, state_second, state_first)
    state_copy = remote(
        pair_states.at[0], pair_states.at[1], pair_send.at[1], pair_recv.at[1], (sibling, tp)
    )
    state_copy.start()

    ones = group_ones(PAIR)

    def read_pair(p, state, half):
        readout = local_rows[p] + dot3(carried_rows[p], diagonal(state))
        scale = lax.rsqrt(dot2(readout * readout, ones) * (1.0 / HEAD) + HEAD_EPS)
        mix_out = (readout * scale * gate_gain[p]).astype(BF16)
        started = []
        for k in range(4):
            mix_sent[half, k] = mix_out[k * 64 : (k + 1) * 64]
        for step in (2, 1, 3):
            copy = remote(
                mix_sent.at[half, x_of(step)], mix_full.at[half, tp],
                mix_send.at[half, step - 1], mix_recv.at[half, step - 1], x_peer(step),
            )
            copy.start()
            started.append(copy)
        return started

    def out_rows(owner, p):
        return pl.ds(pl.multiple_of(owner * 256 + p * PAIR, PAIR), PAIR)

    with jax.named_scope("read_own"):
        started = read_pair(core, mine, 0)

    with jax.named_scope("own_out"):
        loads[3].wait()
        loads[4].wait()
        acc[...] = dot(
            conv_full[0, tp], conv_out_w[pl.ds(pl.multiple_of(tp * PAIR, PAIR), PAIR), :]
        ) + dot(mix_sent[0, tp], mix_out_w[out_rows(tp, core), :])
    with jax.named_scope("state_wait"):
        state_copy.wait()
    with jax.named_scope("read_other"):
        started += read_pair(1 - core, pair_states[1], 1)
    with jax.named_scope("conv_out"):
        for step in (1, 3, 2):
            arrived = x_of(4 - step)
            remote(
                conv_full.at[0, arrived], conv_full.at[1, arrived],
                conv_send.at[step - 1], conv_recv.at[step - 1], x_peer(step),
            ).wait_recv()
            rows = pl.ds(pl.multiple_of(arrived * PAIR, PAIR), PAIR)
            acc[...] += dot(conv_full[1, arrived], conv_out_w[rows, :])
    with jax.named_scope("mix_own"):
        acc[...] += dot(mix_sent[1, tp], mix_out_w[out_rows(tp, 1 - core), :])
    for copy in conv_copies:
        copy.wait_send()
    pl.when(sp < 31)(halo_copy.wait_send)
    for step in (1, 2, 3):
        pl.when(y_sends(step))(lambda step=step: y_copy(step, y, y_target(step)).wait_send())

        @pl.when(z + step < 4)
        def _(step=step):
            z_copy(step, 1, z, sp + 8 * step).wait_send()
            pl.when(z > 0)(z_copy(step, 0, z, sp + 8 * step).wait_send)

        pl.when((y == 3) & (z + step < 4))(
            lambda step=step: raw_copy(step, y, z, raw_target(step)).wait_send()
        )

    for half in (0, 1):
        for step in (1, 3, 2):
            arrived = x_of(4 - step)
            with jax.named_scope("mix_wait"):
                remote(
                    mix_sent.at[half, arrived], mix_full.at[half, arrived],
                    mix_send.at[half, step - 1], mix_recv.at[half, step - 1], x_peer(step),
                ).wait_recv()
            with jax.named_scope("mix_project"):
                p = core if half == 0 else 1 - core
                acc[...] += dot(mix_full[half, arrived], mix_out_w[out_rows(arrived, p), :])
    with jax.named_scope("final"):
        out_ref[...] = acc[...].astype(BF16)
    for copy in started:
        copy.wait_send()


VMEM = pl.BlockSpec(memory_space=pltpu.VMEM)
ANY = pl.BlockSpec(memory_space=pltpu.HBM)


def local(
    tokens, input_norm_gain, convolution_value_weight, convolution_gate_weight,
    depthwise_taps_weight, convolution_group_gain, convolution_group_shift, receptance_weight,
    key_weight, value_weight, decay_weight, correction_rate_weight, output_gate_weight,
    key_prenorm_gain, decay_offset_bias, position_decay_shift, extra_log_decay, head_norm_gain,
    convolution_output_weight, attention_output_weight,
):
    dma = pltpu.SemaphoreType.DMA
    return pl.pallas_call(
        layer_kernel,
        name="layer",
        out_shape=pltpu.VMEM((64, 2048), BF16),
        in_specs=[ANY] * 20,
        out_specs=VMEM,
        scratch_shapes=[
            pltpu.VMEM((1, 2048), F32),
            pltpu.VMEM((1, 256), F32),
            pltpu.VMEM((1, 256), F32),
            pltpu.VMEM((31, 128), F32),
            pltpu.VMEM((1, 128), F32),
            pltpu.VMEM((1, 128), F32),
            pltpu.VMEM((1, 256), F32),
            pltpu.VMEM((256, 2048), BF16),
            pltpu.VMEM((256, 2048), BF16),
            pltpu.VMEM((6, 2048, 256), BF16),
            pltpu.VMEM((256, 256), F32),
            pltpu.VMEM((256, 256), F32),
            pltpu.VMEM((2048, 256), BF16),
            pltpu.VMEM((512, 2048), BF16),
            pltpu.VMEM((1024, 2048), BF16),
            pltpu.VMEM((2, 64, 256), F32),
            pltpu.VMEM((64, 256), F32),
            pltpu.VMEM((2, 64, 128), F32),
            pltpu.VMEM((4, 64, 256), BF16),
            pltpu.VMEM((4, 2, 64, 128), BF16),
            pltpu.VMEM((3, 64, 256), BF16),
            pltpu.VMEM((3, 2, 64, 128), BF16),
            pltpu.VMEM((3, 64, 256), BF16),
            pltpu.VMEM((3, 64, 256), BF16),
            pltpu.VMEM((288, 128), F32),
            pltpu.VMEM((32, 128), BF16),
            pltpu.VMEM((32, 128), BF16),
            pltpu.VMEM((2, 256, 128), F32),
            pltpu.VMEM((2, 256, 128), F32),
            pltpu.VMEM((2, 256, 128), F32),
            pltpu.VMEM((2, 4, 64, 128), BF16),
            pltpu.VMEM((2, 4, 64, 128), BF16),
            pltpu.VMEM((2, 4, 64, 128), BF16),
            pltpu.VMEM((64, 2048), F32),
            dma((8,)), dma((5,)), dma((2,)), dma((2,)), dma((3,)), dma((3,)), dma((3, 2)), dma((3, 2)),
            dma((1,)), dma((1,)), dma((3,)), dma((3,)), dma((2, 3)), dma((2, 3)), dma((7,)), dma((3,)), dma((3,)),
        ],
        compiler_params=pltpu.CompilerParams(
            collective_id=0, has_side_effects=True, vmem_limit_bytes=56000000
        ),
    )(
        *(
            pltpu.with_memory_space_constraint(operand, pltpu.HBM)
            for operand in (
                tokens, input_norm_gain.reshape(1, -1), decay_weight, key_weight,
                correction_rate_weight, receptance_weight, value_weight,
                key_prenorm_gain.reshape(1, -1), decay_offset_bias.reshape(1, -1),
                position_decay_shift, extra_log_decay, convolution_value_weight,
                convolution_gate_weight, output_gate_weight, depthwise_taps_weight,
                convolution_group_gain.reshape(1, -1), convolution_group_shift.reshape(1, -1),
                head_norm_gain.reshape(1, -1), convolution_output_weight, attention_output_weight,
            )
        )
    )


def solution(mesh):
    rows, chans, vec = P("sp", None), P(None, "tp"), P("tp")
    placed = (
        rows, P(), chans, chans, chans, vec, vec, chans, chans, chans, chans, chans, chans,
        vec, vec, P("sp", "tp"), P("sp", "tp"), vec, P(), P(),
    )
    return jax.shard_map(
        local, mesh=mesh, in_specs=placed, out_specs=P(("sp", "tp"), None), check_vma=False
    )
```

```python
import functools

import jax
import jax.numpy as jnp
from jax import lax
from jax.experimental import pallas as pl
from jax.experimental.pallas import tpu as pltpu
from jax.sharding import PartitionSpec as P

F32 = jnp.float32
BF16 = jnp.bfloat16
MESH = pl.DeviceIdType.MESH
HEAD = 64
CHUNK = 64
PAIR = 128

NORM_EPS = 1e-06
GROUP_EPS = 1e-05
HEAD_EPS = 0.00064
KEY_EPS = 1e-06

NN = (((1,), (0,)), ((), ()))
NT = (((1,), (1,)), ((), ()))


def dot(left, right, dims=NN):
    return lax.dot_general(left, right, dims, preferred_element_type=F32)


def split(values):
    high = values.astype(BF16)
    return high, (values - high.astype(F32)).astype(BF16)


def dot1(left, right, dims=NN):
    return dot(left.astype(BF16), right.astype(BF16), dims)


def dot3(left, right, dims=NN):
    left_high, left_low = split(left)
    right_high, right_low = split(right)
    return dot(left_high, right_high, dims) + (
        dot(left_low, right_high, dims) + dot(left_high, right_low, dims)
    )


def dot2(left, right_exact):
    high, low = split(left)
    return dot(high, right_exact) + dot(low, right_exact)


def iota(shape, dim):
    return lax.broadcasted_iota(jnp.int32, shape, dim)


def first_head(rows):
    return iota((rows, PAIR), 1) < HEAD


def diagonal(packed):
    mask = first_head(packed.shape[0])
    return jnp.concatenate([jnp.where(mask, packed, 0.0), jnp.where(mask, 0.0, packed)], axis=0)


def undiagonal(full):
    return jnp.where(first_head(HEAD), full[:HEAD], full[HEAD:])


def beside(*parts):
    return jnp.concatenate(parts, axis=1)


def group_ones(width):
    return (iota((width, width), 0) // HEAD == iota((width, width), 1) // HEAD).astype(BF16)


def sigmoid(values):
    return 1.0 / (1.0 + jnp.exp(-values))


def rounded(values):
    return values.astype(BF16).astype(F32)


def normalize(tokens, gain):
    rows = tokens.astype(F32)
    scale = lax.rsqrt(jnp.mean(rows * rows, axis=-1, keepdims=True) + NORM_EPS)
    return (rows * scale * gain).astype(BF16)


def group_norm(values, ones, eps):
    centred = values - dot2(values, ones) * (1.0 / HEAD)
    return centred * lax.rsqrt(dot2(centred * centred, ones) * (1.0 / HEAD) + eps)


def compose(later, earlier, product):
    trans, base = later
    out = product(trans, beside(diagonal(earlier[0]), diagonal(earlier[1])))
    return out[:, :PAIR], out[:, PAIR:] + base


def chunk_algebra(receptance, key, value, decay, rate, key_gain, decay_bias, shift, extra):
    tok_rows, width = receptance.shape
    chunks, pairs = tok_rows // CHUNK, width // PAIR
    logits = decay + decay_bias + shift
    log_decay = sigmoid(logits) * (-0.6065306597126334) + extra
    scaled = key * key_gain
    ones = group_ones(width)
    unit = scaled * lax.rsqrt(dot2(scaled * scaled, ones) + KEY_EPS)
    erase = unit * sigmoid(rate)
    value = value - dot(value.astype(BF16), ones) * (1.0 / HEAD)
    row, col = iota((tok_rows, tok_rows), 0), iota((tok_rows, tok_rows), 1)
    running = ((row // CHUNK == col // CHUNK) & (row >= col)).astype(BF16)
    high, low = split(log_decay)
    total = dot(running, high) + dot(running, low)

    strict_rows = iota((CHUNK, PAIR), 0)
    strict_cols = iota((CHUNK, PAIR), 1) % HEAD
    strict = strict_rows > strict_cols
    inclusive = strict_rows >= strict_cols
    eye = (strict_rows == strict_cols).astype(F32)
    same8 = (strict_rows // 8) == (strict_cols // 8)
    lane_first = first_head(CHUNK)

    units = []
    for c in range(chunks):
        rows = slice(c * CHUNK, (c + 1) * CHUNK)
        cum = total[rows]
        last = cum[CHUNK - 1 : CHUNK]
        half = 0.5 * last
        grow = jnp.exp(half - cum)
        shrink = jnp.exp(cum - half)
        half_decay = jnp.exp(half)
        query_unit = unit[rows] * jnp.exp(cum - log_decay[rows] - half)
        query_read = receptance[rows] * shrink
        scaled_erase = erase[rows] * grow
        scaled_key = key[rows] * grow
        for p in range(pairs):
            lanes = slice(p * PAIR, (p + 1) * PAIR)
            units.append(
                dict(
                    c=c,
                    p=p,
                    qu=query_unit[:, lanes],
                    qr=query_read[:, lanes],
                    se=scaled_erase[:, lanes],
                    sk=scaled_key[:, lanes],
                    v=value[rows, lanes],
                    half=half_decay[:, lanes],
                )
            )
    for u in units:
        left = jnp.concatenate([u["qu"], u["qr"]], axis=0)
        right = jnp.concatenate([diagonal(u["se"]), diagonal(u["sk"])], axis=0)
        u["gram"] = dot1(left, right, NT)
    for u in units:
        gram = u.pop("gram")
        u["mix"] = jnp.where(strict, gram[:CHUNK, :PAIR], 0.0)
        u["key_mix"] = jnp.where(strict, gram[:CHUNK, PAIR:], 0.0)
        u["read_erase"] = jnp.where(inclusive, gram[CHUNK:, :PAIR], 0.0)
        u["read_key"] = jnp.where(inclusive, gram[CHUNK:, PAIR:], 0.0)
        u["near"] = jnp.where(same8, u["mix"], 0.0)
        u["far"] = jnp.where(same8, 0.0, u["mix"])
    for u in units:
        u["near2"] = dot3(u["near"], diagonal(u["near"]))
        u["value_part"] = dot1(
            jnp.concatenate([u.pop("key_mix"), u.pop("read_key")], axis=0), diagonal(u["v"])
        )
    for u in units:
        powers = dot3(jnp.concatenate([u["near"], u["near2"]], axis=0), diagonal(u["near2"]))
        u["start"] = eye - u.pop("near") + u.pop("near2") - powers[:CHUNK]
        u["near4"] = powers[CHUNK:]
    for u in units:
        u["inv8"] = u["start"] + dot3(u["start"], diagonal(u.pop("near4")))
        u.pop("start")
    for u in units:
        right = beside(
            diagonal(u.pop("far")), diagonal(u["value_part"][:CHUNK]), diagonal(u["qu"] * u["half"])
        )
        out = dot1(u.pop("inv8"), right)
        u["step"], u["removed"] = out[:, :PAIR], -out[:, PAIR:]
    for sign, last in ((-1.0, False), (1.0, False), (1.0, True)):
        for u in units:
            step, removed = u.pop("step"), u["removed"]
            parts = [diagonal(removed[:, :PAIR]), diagonal(removed[:, PAIR:])]
            if not last:
                parts.append(diagonal(step))
            out = dot1(step, beside(*parts))
            u["removed"] = removed + sign * out[:, : 2 * PAIR]
            if not last:
                u["step"] = out[:, 2 * PAIR :]
    for u in units:
        kept = jnp.concatenate([u["se"] * u["half"], u["sk"] * u["half"]], axis=0)
        right = jnp.concatenate(
            [u["removed"], beside(u["v"], jnp.zeros_like(u["v"]))], axis=0
        )
        out = dot1(kept.T, right)
        u["base"] = undiagonal(out[:, :PAIR])
        u["trans"] = undiagonal(out[:, PAIR:]) + eye * (u["half"] * u["half"])
    return units


def local_reads(units):
    for u in units:
        removed = u["removed"]
        right = beside(diagonal(removed[:, :PAIR]), diagonal(removed[:, PAIR:]))
        out = dot1(u["read_erase"], right)
        u["local"] = out[:, :PAIR] + u["value_part"][CHUNK:]
        u["carried"] = out[:, PAIR:] + u["qr"] * u["half"]


def layer_kernel(
    tokens_hbm, gain_hbm, decay_hbm, key_hbm, rate_hbm, receptance_hbm, value_hbm,
    key_gain_hbm, bias_hbm, shift_hbm, extra_hbm,
    conv_value_hbm, conv_gate_hbm, gate_hbm, taps_hbm, group_gain_hbm, group_shift_hbm,
    head_gain_hbm, conv_out_hbm, mix_out_hbm,
    out_ref,
    gain_ref, key_gain_ref, bias_ref, taps_ref, group_gain_ref, group_shift_ref, head_gain_ref,
    tokens, normed, weights, shift, extra, gate_w, conv_out_w, mix_out_w,
    totals, peer_total, pair_states, y_slots, z_slots, y_seen, z_seen, raw_slots, raw_seen, extended, halo, conv_rows,
    local_rows, carried_rows, gate_gain, conv_full, mix_sent, mix_full, acc,
    sems, pair_send, pair_recv, y_send, y_recv, z_send, z_recv, halo_send, halo_recv,
    conv_send, conv_recv, mix_send, mix_recv, raw_send, raw_recv,
):
    sp, tp = lax.axis_index("sp"), lax.axis_index("tp")
    core = lax.rem(sp, 2)
    y = lax.rem(sp // 2, 4)
    z = sp // 8
    sibling = sp + 1 - 2 * core
    after = lax.rem(sp + 1, 32)
    is_first = core == 0

    def y_source(step):
        return z * 8 + lax.rem(y + 4 - step, 4) * 2 + core

    def y_target(step):
        return z * 8 + lax.rem(y + step, 4) * 2 + core

    def x_of(step):
        return lax.rem(tp + step, 4)

    def x_peer(step):
        return (sp, x_of(step))

    def remote(source, target, send, recv, peer):
        return pltpu.make_async_remote_copy(
            src_ref=source, dst_ref=target, send_sem=send, recv_sem=recv,
            device_id=peer, device_id_type=MESH,
        )

    order = (decay_hbm, key_hbm, rate_hbm, receptance_hbm, value_hbm)
    def load(source, target, k):
        return pltpu.make_async_copy(source, target, sems.at[k])

    copies = [load(tokens_hbm, tokens, 0)]
    for i, source in enumerate(order):
        copies.append(load(source, weights.at[i], 1 + i))
    late = [load(shift_hbm, shift, 6), load(extra_hbm, extra, 7)]
    gain_copy = load(gain_hbm, gain_ref, 8)
    smalls = [load(key_gain_hbm, key_gain_ref, 0), load(bias_hbm, bias_ref, 8)]
    rest = [
        load(taps_hbm, taps_ref, 1),
        load(group_gain_hbm, group_gain_ref, 2),
        load(group_shift_hbm, group_shift_ref, 3),
        load(head_gain_hbm, head_gain_ref, 4),
    ]
    copies[0].start()
    gain_copy.start()
    for copy in copies[1:] + late:
        copy.start()

    barrier = pltpu.get_barrier_semaphore()

    def greet(peer):
        pl.semaphore_signal(barrier, inc=1, device_id=peer, device_id_type=MESH)

    greet((sibling, tp))
    pl.when(sp > 0)(lambda: greet((sp - 1, tp)))
    for step in (1, 2, 3):
        meets = (step <= y) | ((z < 3) & (y > 0)) if step == 1 else (step <= y) | (z < 3)
        pl.when(meets)(lambda step=step: greet((y_source(step), tp)))
        pl.when((y == 0) & (step <= z))(
            lambda step=step: greet(((z - step) * 8 + 6 + core, tp))
        )
        pl.when(step <= z)(lambda step=step: greet((sp - 8 * step, tp)))
        greet(x_peer(step))
    targets = (
        4 + jnp.where(sp < 31, 1, 0) + jnp.where(z < 3, jnp.where(y == 3, 2, 3), 3 - y) + (3 - z)
        + jnp.where(y == 3, 3 - z, 0)
    )

    loads = [
        load(gate_hbm, gate_w, 0),
        load(conv_value_hbm, weights.at[5, :, pl.ds(0, PAIR)], 8),
        load(conv_gate_hbm, weights.at[5, :, pl.ds(PAIR, PAIR)], 5),
        load(conv_out_hbm, conv_out_w, 6),
        load(mix_out_hbm, mix_out_w, 7),
    ]
    eye = (iota((HEAD, 2 * PAIR), 0) == iota((HEAD, 2 * PAIR), 1) % HEAD) & (
        iota((HEAD, 2 * PAIR), 1) < PAIR
    )
    identity = jnp.where(eye, 1.0, 0.0).astype(BF16)
    for k in range(3):
        y_seen[k] = identity
        raw_seen[k] = identity
        z_seen[k, 0] = identity[:, :PAIR]
        z_seen[k, 1] = identity[:, PAIR:]
    with jax.named_scope("wait_tokens"):
        copies[0].wait()
        gain_copy.wait()
        for copy in smalls:
            copy.start()
    with jax.named_scope("norm"):
        normed[...] = normalize(tokens[...], gain_ref[...])
    with jax.named_scope("project"):
        found = []
        for i in (0, 2):
            copies[1 + i].wait()
            copies[2 + i].wait()
            found.append(dot(normed[...], weights[i]))
            found.append(dot(normed[...], weights[i + 1]))
        copies[5].wait()
        half = weights.shape[1] // 2
        keep = jnp.where(sp < 32, 1.0, 0.0)
        found.append(
            dot(normed[:, :half], weights[4, :half, :])
            + keep * dot(normed[:, half:], weights[4, half:, :])
        )
        decay, key, rate, receptance, value = (rounded(rows) for rows in found)
        for copy in late + smalls:
            copy.wait()
    for copy in loads[:3] + rest + loads[3:]:
        copy.start()
    with jax.named_scope("algebra"):
        units = chunk_algebra(
            receptance, key, value, decay, rate, key_gain_ref[...], bias_ref[...], shift[...],
            extra[...],
        )
    with jax.named_scope("totals"):
        prefixes = []
        for p in range(2):
            steps = [(u["trans"], u["base"]) for u in units if u["p"] == p]
            two = compose(steps[1], steps[0], dot3)
            upper = compose(steps[3], steps[2], dot3)
            totals[p] = beside(*compose(upper, two, dot3))
            prefixes.append((steps[0], two, steps[2]))
    with jax.named_scope("barrier"):
        pl.semaphore_wait(barrier, targets)
    pair_copy = remote(
        totals.at[1 - core], peer_total, pair_send.at[0], pair_recv.at[0], (sibling, tp)
    )
    pair_copy.start()

    with jax.named_scope("conv_project"):
        for copy in loads[:3]:
            copy.wait()
        gate_rows = dot(normed[...], gate_w[...])
        conv_both = rounded(dot(normed[...], weights[5]))
        conv_input = (conv_both[:, :PAIR] * sigmoid(conv_both[:, PAIR:])).astype(BF16)
        conv_rows[...] = conv_input[224:]
        halo_copy = remote(conv_rows, halo, halo_send.at[0], halo_recv.at[0], (after, tp))
        pl.when(sp < 31)(halo_copy.start)
        extended[:32, :] = jnp.zeros((32, PAIR), F32)
        extended[32:, :] = conv_input.astype(F32)

    with jax.named_scope("gate_project"):
        for copy in rest:
            copy.wait()
        gated = sigmoid(rounded(gate_rows)) * head_gain_ref[...]
        gate_gain[0] = gated[:, :PAIR]
        gate_gain[1] = gated[:, PAIR:]
    with jax.named_scope("pair_wait"):
        pair_copy.wait()
    with jax.named_scope("pair_compose"):
        own, other = totals[core], peer_total[...]
        first = jnp.where(is_first, own, other)
        second = jnp.where(is_first, other, own)
        chip_first = (first[:, :PAIR], first[:, PAIR:])
        chip = compose((second[:, :PAIR], second[:, PAIR:]), chip_first, dot3)
        y_slots[y] = beside(*chip).astype(BF16)

    def y_copy(step, slot, peer):
        return remote(
            y_slots.at[slot], y_slots.at[slot], y_send.at[step - 1], y_recv.at[step - 1],
            (peer, tp),
        )

    def raw_copy(up, slot, plane, peer):
        return remote(
            y_slots.at[slot], raw_slots.at[plane], raw_send.at[up - 1], raw_recv.at[plane],
            (peer, tp),
        )

    def raw_target(up):
        return (z + up) * 8 + core

    for up in (1, 2, 3):
        pl.when((y == 3) & (z + up < 4))(
            lambda up=up: raw_copy(up, y, z, raw_target(up)).start()
        )

    def y_sends(step):
        return (y + step < 4) | ((z < 3) & (y < 3)) if step == 1 else (y + step < 4) | (z < 3)

    for step in (2, 3, 1):
        pl.when(y_sends(step))(lambda step=step: y_copy(step, y, y_target(step)).start())

    with jax.named_scope("local_reads"):
        local_reads(units)
        for p in range(2):
            one, two, third = prefixes[p]
            earlier = (None, one, two, compose(third, two, dot1))
            for u in units:
                if u["p"] != p:
                    continue
                c = u["c"]
                rows = slice(c * CHUNK, (c + 1) * CHUNK)
                if c == 0:
                    local_rows[p, rows] = u["local"]
                    carried_rows[p, rows] = u["carried"]
                    continue
                right = beside(diagonal(earlier[c][0]), diagonal(earlier[c][1]))
                out = dot1(u["carried"], right)
                carried_rows[p, rows] = out[:, :PAIR]
                local_rows[p, rows] = out[:, PAIR:] + u["local"]

    with jax.named_scope("y_wait_lower"):
        for step in (1, 2, 3):

            @pl.when(step <= y)
            def _(step=step):
                y_copy(step, y - step, sibling).wait_recv()
                y_seen[y - step] = y_slots[y - step]

    def slot(ref, k):
        both = ref[k].astype(F32)
        return both[:, :PAIR], both[:, PAIR:]

    with jax.named_scope("before_chip"):
        before_chip = compose(
            slot(y_seen, 2), compose(slot(y_seen, 1), slot(y_seen, 0), dot1), dot3
        )
        before_second = compose(chip_first, before_chip, dot3)
        trans_both = jnp.concatenate([before_chip[0], before_second[0]], axis=0)
        base_both = jnp.concatenate([before_chip[1], before_second[1]], axis=0)

    with jax.named_scope("halo_wait"):

        @pl.when(sp > 0)
        def _():
            halo_copy.wait_recv()
            extended[:32, :] = halo[...].astype(F32)

    with jax.named_scope("convolution"):
        taps = taps_ref[...]
        conv_sum = jnp.zeros((256, PAIR), F32)
        for j in range(31):
            conv_sum = conv_sum + taps[j : j + 1] * extended[pl.ds(2 + j, 256), :]
        normal = group_norm(conv_sum, group_ones(PAIR), GROUP_EPS)
        affine = normal * group_gain_ref[...] + group_shift_ref[...]
        conv_out = (affine * sigmoid(affine)).astype(BF16)
        for k in range(4):
            conv_full[0, k] = conv_out[k * 64 : (k + 1) * 64]
    for step in (2, 1, 3):
        copy = remote(
            conv_full.at[0, x_of(step)], conv_full.at[1, tp],
            conv_send.at[0], conv_recv.at[0], x_peer(step),
        )
        copy.start()

    def z_copy(up, slot, peer, whole):
        part = z_slots.at[slot] if whole else z_slots.at[slot, 1]
        return remote(part, part, z_send.at[up - 1], z_recv.at[slot], (peer, tp))

    def z_column(up):
        pl.when(z > 0)(lambda: z_copy(up, z, sp + 8 * up, True).start())
        pl.when(z == 0)(lambda: z_copy(up, z, sp + 8 * up, False).start())

    def upper(step):
        y_copy(step, lax.rem(y + 4 - step, 4), sibling).wait_recv()

    with jax.named_scope("plane"):

        @pl.when(z < 3)
        def _():
            for step in (3, 2):
                pl.when(step > y)(lambda step=step: upper(step))
            lower = compose(slot(y_slots, 1), slot(y_slots, 0), dot1)

            def store(total):
                z_slots[z, 0] = total[0].astype(BF16)
                z_slots[z, 1] = total[1].astype(BF16)

            @pl.when(y == 0)
            def _():
                store(compose(slot(y_slots, 2), lower, dot3))

            @pl.when(y > 0)
            def _():
                store(compose(compose(slot(y_slots, 3), slot(y_slots, 2), dot1), lower, dot3))

            z_column(1)
            pl.when(z < 2)(lambda: z_column(2))
            pl.when(z < 1)(lambda: z_column(3))

    def z_arrival(below):
        pl.when(below > 0)(lambda: z_copy(1, below, sibling, True).wait_recv())
        pl.when(below == 0)(lambda: z_copy(1, below, sibling, False).wait_recv())

    with jax.named_scope("z_wait"):
        for below in range(2):

            @pl.when(below < z - 1)
            def _(below=below):
                z_arrival(below)
                if below > 0:
                    z_seen[below, 0] = z_slots[below, 0]
                z_seen[below, 1] = z_slots[below, 1]

        for below in range(3):

            @pl.when((y == 0) & (below < z))
            def _(below=below):
                raw_copy(1, 0, below, sibling).wait_recv()
                raw_seen[jnp.where(below < z - 1, below, 2)] = raw_slots[below]

        def through(parts, state):
            return dot3(parts[0], diagonal(state)) + parts[1]

        def plane_below(k):
            return z_seen[k, 0].astype(F32), z_seen[k, 1].astype(F32)

        far = through(slot(raw_seen, 0), z_seen[0, 1].astype(F32))
        far = through(slot(raw_seen, 1), through(plane_below(1), far))
        passed = raw_seen[2]
        out = dot3(
            trans_both,
            beside(
                diagonal(passed[:, :PAIR].astype(F32)), diagonal(passed[:, PAIR:].astype(F32))
            ),
        )
        trans_last, base_last = out[:, :PAIR], out[:, PAIR:] + base_both

        @pl.when(z > 0)
        def _():
            z_arrival(z - 1)

            @pl.when(z > 1)
            def _():
                z_seen[2, 0] = z_slots[z - 1, 0]

            z_seen[2, 1] = z_slots[z - 1, 1]

    with jax.named_scope("z_compose"):
        entering = through(plane_below(2), far)
        states = dot3(trans_last, diagonal(entering)) + base_last
        state_first, state_second = states[:HEAD], states[HEAD:]
        mine = jnp.where(is_first, state_first, state_second)
        pair_states[0] = jnp.where(is_first, state_second, state_first)
    state_copy = remote(
        pair_states.at[0], pair_states.at[1], pair_send.at[0], pair_recv.at[1], (sibling, tp)
    )
    state_copy.start()

    ones = group_ones(PAIR)

    def read_pair(p, state, half):
        readout = local_rows[p] + dot3(carried_rows[p], diagonal(state))
        scale = lax.rsqrt(dot2(readout * readout, ones) * (1.0 / HEAD) + HEAD_EPS)
        mix_out = (readout * scale * gate_gain[p]).astype(BF16)
        for k in range(4):
            mix_sent[half, k] = mix_out[k * 64 : (k + 1) * 64]
        for step in (2, 1, 3):
            copy = remote(
                mix_sent.at[half, x_of(step)], mix_full.at[half, tp],
                mix_send.at[half], mix_recv.at[half, step - 1], x_peer(step),
            )
            copy.start()

    def out_rows(owner, p):
        return pl.ds(pl.multiple_of(owner * 256 + p * PAIR, PAIR), PAIR)

    with jax.named_scope("read_own"):
        read_pair(core, mine, 0)

    with jax.named_scope("own_out"):
        loads[3].wait()
        loads[4].wait()
        acc[...] = dot(
            conv_full[0, tp], conv_out_w[pl.ds(pl.multiple_of(tp * PAIR, PAIR), PAIR), :]
        ) + dot(mix_sent[0, tp], mix_out_w[out_rows(tp, core), :])
    with jax.named_scope("state_wait"):
        state_copy.wait()
    with jax.named_scope("read_other"):
        read_pair(1 - core, pair_states[1], 1)
    conv_all = remote(
        conv_full.at[0, pl.ds(0, 3)], conv_full.at[1, pl.ds(0, 3)], conv_send.at[0],
        conv_recv.at[0], x_peer(1),
    )
    with jax.named_scope("conv_out"):
        conv_all.wait_recv()
        for step in (1, 3, 2):
            arrived = x_of(4 - step)
            rows = pl.ds(pl.multiple_of(arrived * PAIR, PAIR), PAIR)
            acc[...] += dot(conv_full[1, arrived], conv_out_w[rows, :])
    with jax.named_scope("mix_own"):
        acc[...] += dot(mix_sent[1, tp], mix_out_w[out_rows(tp, 1 - core), :])
    conv_all.wait_send()
    pl.when(sp < 31)(halo_copy.wait_send)
    for step in (1, 2, 3):
        pl.when(y_sends(step))(lambda step=step: y_copy(step, y, y_target(step)).wait_send())

        @pl.when(z + step < 4)
        def _(step=step):
            pl.when(z > 0)(lambda: z_copy(step, z, sp + 8 * step, True).wait_send())
            pl.when(z == 0)(lambda: z_copy(step, z, sp + 8 * step, False).wait_send())

        pl.when((y == 3) & (z + step < 4))(
            lambda step=step: raw_copy(step, y, z, raw_target(step)).wait_send()
        )

    for half in (0, 1):
        for step in (1, 3, 2):
            arrived = x_of(4 - step)
            with jax.named_scope("mix_wait"):
                remote(
                    mix_sent.at[half, arrived], mix_full.at[half, arrived],
                    mix_send.at[half], mix_recv.at[half, step - 1], x_peer(step),
                ).wait_recv()
            with jax.named_scope("mix_project"):
                p = core if half == 0 else 1 - core
                acc[...] += dot(mix_full[half, arrived], mix_out_w[out_rows(arrived, p), :])
    with jax.named_scope("final"):
        out_ref[...] = acc[...].astype(BF16)
    for half in (0, 1):
        block = mix_sent.at[half, pl.ds(0, 3)]
        remote(block, block, mix_send.at[half], mix_recv.at[half, 0], x_peer(1)).wait_send()


VMEM = pl.BlockSpec(memory_space=pltpu.VMEM)
ANY = pl.BlockSpec(memory_space=pltpu.HBM)


def local(
    tokens, input_norm_gain, convolution_value_weight, convolution_gate_weight,
    depthwise_taps_weight, convolution_group_gain, convolution_group_shift, receptance_weight,
    key_weight, value_weight, decay_weight, correction_rate_weight, output_gate_weight,
    key_prenorm_gain, decay_offset_bias, position_decay_shift, extra_log_decay, head_norm_gain,
    convolution_output_weight, attention_output_weight,
):
    dma = pltpu.SemaphoreType.DMA
    return pl.pallas_call(
        layer_kernel,
        name="layer",
        out_shape=pltpu.VMEM((64, 2048), BF16),
        in_specs=[ANY] * 20,
        out_specs=VMEM,
        scratch_shapes=[
            pltpu.VMEM((1, 2048), F32),
            pltpu.VMEM((1, 256), F32),
            pltpu.VMEM((1, 256), F32),
            pltpu.VMEM((31, 128), F32),
            pltpu.VMEM((1, 128), F32),
            pltpu.VMEM((1, 128), F32),
            pltpu.VMEM((1, 256), F32),
            pltpu.VMEM((256, 2048), BF16),
            pltpu.VMEM((256, 2048), BF16),
            pltpu.VMEM((6, 2048, 256), BF16),
            pltpu.VMEM((256, 256), F32),
            pltpu.VMEM((256, 256), F32),
            pltpu.VMEM((2048, 256), BF16),
            pltpu.VMEM((512, 2048), BF16),
            pltpu.VMEM((1024, 2048), BF16),
            pltpu.VMEM((2, 64, 256), F32),
            pltpu.VMEM((64, 256), F32),
            pltpu.VMEM((2, 64, 128), F32),
            pltpu.VMEM((4, 64, 256), BF16),
            pltpu.VMEM((4, 2, 64, 128), BF16),
            pltpu.VMEM((3, 64, 256), BF16),
            pltpu.VMEM((3, 2, 64, 128), BF16),
            pltpu.VMEM((3, 64, 256), BF16),
            pltpu.VMEM((3, 64, 256), BF16),
            pltpu.VMEM((288, 128), F32),
            pltpu.VMEM((32, 128), BF16),
            pltpu.VMEM((32, 128), BF16),
            pltpu.VMEM((2, 256, 128), F32),
            pltpu.VMEM((2, 256, 128), F32),
            pltpu.VMEM((2, 256, 128), F32),
            pltpu.VMEM((2, 4, 64, 128), BF16),
            pltpu.VMEM((2, 4, 64, 128), BF16),
            pltpu.VMEM((2, 4, 64, 128), BF16),
            pltpu.VMEM((64, 2048), F32),
            dma((9,)), dma((1,)), dma((2,)), dma((3,)), dma((3,)), dma((3,)), dma((3,)),
            dma((1,)), dma((1,)), dma((1,)), dma((1,)), dma((2,)), dma((2, 3)), dma((3,)), dma((3,)),
        ],
        compiler_params=pltpu.CompilerParams(
            collective_id=0, has_side_effects=True, vmem_limit_bytes=56000000
        ),
    )(
        *(
            pltpu.with_memory_space_constraint(operand, pltpu.HBM)
            for operand in (
                tokens, input_norm_gain.reshape(1, -1), decay_weight, key_weight,
                correction_rate_weight, receptance_weight, value_weight,
                key_prenorm_gain.reshape(1, -1), decay_offset_bias.reshape(1, -1),
                position_decay_shift, extra_log_decay, convolution_value_weight,
                convolution_gate_weight, output_gate_weight, depthwise_taps_weight,
                convolution_group_gain.reshape(1, -1), convolution_group_shift.reshape(1, -1),
                head_norm_gain.reshape(1, -1), convolution_output_weight, attention_output_weight,
            )
        )
    )


def solution(mesh):
    rows, chans, vec = P("sp", None), P(None, "tp"), P("tp")
    placed = (
        rows, P(), chans, chans, chans, vec, vec, chans, chans, chans, chans, chans, chans,
        vec, vec, P("sp", "tp"), P("sp", "tp"), vec, P(), P(),
    )
    return jax.shard_map(
        local, mesh=mesh, in_specs=placed, out_specs=P(("sp", "tp"), None), check_vma=False
    )
```

```python
import functools

import jax
import jax.numpy as jnp
from jax import lax
from jax.experimental import pallas as pl
from jax.experimental.pallas import tpu as pltpu
from jax.sharding import PartitionSpec as P

F32 = jnp.float32
BF16 = jnp.bfloat16
MESH = pl.DeviceIdType.MESH
HEAD = 64
CHUNK = 64
PAIR = 128

NORM_EPS = 1e-06
GROUP_EPS = 1e-05
HEAD_EPS = 0.00064
KEY_EPS = 1e-06

NN = (((1,), (0,)), ((), ()))
NT = (((1,), (1,)), ((), ()))


def dot(left, right, dims=NN):
    return lax.dot_general(left, right, dims, preferred_element_type=F32)


def split(values):
    high = values.astype(BF16)
    return high, (values - high.astype(F32)).astype(BF16)


def dot1(left, right, dims=NN):
    return dot(left.astype(BF16), right.astype(BF16), dims)


def dot3(left, right, dims=NN):
    left_high, left_low = split(left)
    right_high, right_low = split(right)
    return dot(left_high, right_high, dims) + (
        dot(left_low, right_high, dims) + dot(left_high, right_low, dims)
    )


def dot2(left, right_exact):
    high, low = split(left)
    return dot(high, right_exact) + dot(low, right_exact)


def iota(shape, dim):
    return lax.broadcasted_iota(jnp.int32, shape, dim)


def first_head(rows):
    return iota((rows, PAIR), 1) < HEAD


def diagonal(packed):
    mask = first_head(packed.shape[0])
    return jnp.concatenate([jnp.where(mask, packed, 0.0), jnp.where(mask, 0.0, packed)], axis=0)


def undiagonal(full):
    return jnp.where(first_head(HEAD), full[:HEAD], full[HEAD:])


def beside(*parts):
    return jnp.concatenate(parts, axis=1)


def group_ones(width):
    return (iota((width, width), 0) // HEAD == iota((width, width), 1) // HEAD).astype(BF16)


def sigmoid(values):
    return 1.0 / (1.0 + jnp.exp(-values))


def rounded(values):
    return values.astype(BF16).astype(F32)


def normalize(tokens, gain):
    rows = tokens.astype(F32)
    scale = lax.rsqrt(jnp.mean(rows * rows, axis=-1, keepdims=True) + NORM_EPS)
    return (rows * scale * gain).astype(BF16)


def group_norm(values, ones, eps):
    centred = values - dot2(values, ones) * (1.0 / HEAD)
    return centred * lax.rsqrt(dot2(centred * centred, ones) * (1.0 / HEAD) + eps)


def compose(later, earlier, product):
    trans, base = later
    out = product(trans, beside(diagonal(earlier[0]), diagonal(earlier[1])))
    return out[:, :PAIR], out[:, PAIR:] + base


def chunk_algebra(receptance, key, value, decay, rate, key_gain, decay_bias, shift, extra):
    tok_rows, width = receptance.shape
    chunks, pairs = tok_rows // CHUNK, width // PAIR
    logits = decay + decay_bias + shift
    log_decay = sigmoid(logits) * (-0.6065306597126334) + extra
    scaled = key * key_gain
    ones = group_ones(width)
    unit = scaled * lax.rsqrt(dot2(scaled * scaled, ones) + KEY_EPS)
    erase = unit * sigmoid(rate)
    value = value - dot(value.astype(BF16), ones) * (1.0 / HEAD)
    row, col = iota((tok_rows, tok_rows), 0), iota((tok_rows, tok_rows), 1)
    running = ((row // CHUNK == col // CHUNK) & (row >= col)).astype(BF16)
    high, low = split(log_decay)
    total = dot(running, high) + dot(running, low)

    strict_rows = iota((CHUNK, PAIR), 0)
    strict_cols = iota((CHUNK, PAIR), 1) % HEAD
    strict = strict_rows > strict_cols
    inclusive = strict_rows >= strict_cols
    eye = (strict_rows == strict_cols).astype(F32)
    same8 = (strict_rows // 8) == (strict_cols // 8)
    lane_first = first_head(CHUNK)

    units = []
    for c in range(chunks):
        rows = slice(c * CHUNK, (c + 1) * CHUNK)
        cum = total[rows]
        last = cum[CHUNK - 1 : CHUNK]
        half = 0.5 * last
        grow = jnp.exp(half - cum)
        shrink = jnp.exp(cum - half)
        half_decay = jnp.exp(half)
        query_unit = unit[rows] * jnp.exp(cum - log_decay[rows] - half)
        query_read = receptance[rows] * shrink
        scaled_erase = erase[rows] * grow
        scaled_key = key[rows] * grow
        for p in range(pairs):
            lanes = slice(p * PAIR, (p + 1) * PAIR)
            units.append(
                dict(
                    c=c,
                    p=p,
                    qu=query_unit[:, lanes],
                    qr=query_read[:, lanes],
                    se=scaled_erase[:, lanes],
                    sk=scaled_key[:, lanes],
                    v=value[rows, lanes],
                    half=half_decay[:, lanes],
                )
            )
    for u in units:
        left = jnp.concatenate([u["qu"], u["qr"]], axis=0)
        right = jnp.concatenate([diagonal(u["se"]), diagonal(u["sk"])], axis=0)
        u["gram"] = dot1(left, right, NT)
    for u in units:
        gram = u.pop("gram")
        u["mix"] = jnp.where(strict, gram[:CHUNK, :PAIR], 0.0)
        u["key_mix"] = jnp.where(strict, gram[:CHUNK, PAIR:], 0.0)
        u["read_erase"] = jnp.where(inclusive, gram[CHUNK:, :PAIR], 0.0)
        u["read_key"] = jnp.where(inclusive, gram[CHUNK:, PAIR:], 0.0)
        u["near"] = jnp.where(same8, u["mix"], 0.0)
        u["far"] = jnp.where(same8, 0.0, u["mix"])
    for u in units:
        u["near2"] = dot3(u["near"], diagonal(u["near"]))
        u["value_part"] = dot1(
            jnp.concatenate([u.pop("key_mix"), u.pop("read_key")], axis=0), diagonal(u["v"])
        )
    for u in units:
        powers = dot3(jnp.concatenate([u["near"], u["near2"]], axis=0), diagonal(u["near2"]))
        u["start"] = eye - u.pop("near") + u.pop("near2") - powers[:CHUNK]
        u["near4"] = powers[CHUNK:]
    for u in units:
        u["inv8"] = u["start"] + dot3(u["start"], diagonal(u.pop("near4")))
        u.pop("start")
    for u in units:
        right = beside(
            diagonal(u.pop("far")), diagonal(u["value_part"][:CHUNK]), diagonal(u["qu"] * u["half"])
        )
        out = dot1(u.pop("inv8"), right)
        u["step"], u["removed"] = out[:, :PAIR], -out[:, PAIR:]
    for sign, last in ((-1.0, False), (1.0, False), (1.0, True)):
        for u in units:
            step, removed = u.pop("step"), u["removed"]
            parts = [diagonal(removed[:, :PAIR]), diagonal(removed[:, PAIR:])]
            if not last:
                parts.append(diagonal(step))
            out = dot1(step, beside(*parts))
            u["removed"] = removed + sign * out[:, : 2 * PAIR]
            if not last:
                u["step"] = out[:, 2 * PAIR :]
    for u in units:
        kept = jnp.concatenate([u["se"] * u["half"], u["sk"] * u["half"]], axis=0)
        right = jnp.concatenate(
            [u["removed"], beside(u["v"], jnp.zeros_like(u["v"]))], axis=0
        )
        out = dot1(kept.T, right)
        u["base"] = undiagonal(out[:, :PAIR])
        u["trans"] = undiagonal(out[:, PAIR:]) + eye * (u["half"] * u["half"])
    return units


def local_reads(units):
    for u in units:
        removed = u["removed"]
        right = beside(diagonal(removed[:, :PAIR]), diagonal(removed[:, PAIR:]))
        out = dot1(u["read_erase"], right)
        u["local"] = out[:, :PAIR] + u["value_part"][CHUNK:]
        u["carried"] = out[:, PAIR:] + u["qr"] * u["half"]


def layer_kernel(
    tokens_hbm, gain_hbm, decay_hbm, key_hbm, rate_hbm, receptance_hbm, value_hbm,
    key_gain_hbm, bias_hbm, shift_hbm, extra_hbm,
    conv_value_hbm, conv_gate_hbm, gate_hbm, taps_hbm, group_gain_hbm, group_shift_hbm,
    head_gain_hbm, conv_out_hbm, mix_out_hbm,
    out_ref,
    gain_ref, key_gain_ref, bias_ref, taps_ref, group_gain_ref, group_shift_ref, head_gain_ref,
    tokens, normed, weights, shift, extra, gate_w, conv_out_w, mix_out_w,
    totals, peer_total, pair_states, y_slots, z_slots, y_seen, z_seen, raw_slots, raw_seen, extended, halo, conv_rows,
    local_rows, carried_rows, gate_gain, conv_full, mix_sent, mix_full, acc,
    sems, pair_send, pair_recv, y_send, y_recv, z_send, z_recv, halo_send, halo_recv,
    conv_send, conv_recv, mix_send, mix_recv, raw_send, raw_recv,
):
    sp, tp = lax.axis_index("sp"), lax.axis_index("tp")
    core = lax.rem(sp, 2)
    y = lax.rem(sp // 2, 4)
    z = sp // 8
    sibling = sp + 1 - 2 * core
    after = lax.rem(sp + 1, 32)
    is_first = core == 0

    def y_source(step):
        return z * 8 + lax.rem(y + 4 - step, 4) * 2 + core

    def y_target(step):
        return z * 8 + lax.rem(y + step, 4) * 2 + core

    def x_of(step):
        return lax.rem(tp + step, 4)

    def x_peer(step):
        return (sp, x_of(step))

    def remote(source, target, send, recv, peer):
        return pltpu.make_async_remote_copy(
            src_ref=source, dst_ref=target, send_sem=send, recv_sem=recv,
            device_id=peer, device_id_type=MESH,
        )

    order = (decay_hbm, key_hbm, rate_hbm, receptance_hbm, value_hbm)
    def load(source, target, k):
        return pltpu.make_async_copy(source, target, sems.at[k])

    upper_rows, lower_rows = pl.ds(0, 128), pl.ds(128, 128)
    copies = [load(tokens_hbm.at[upper_rows], tokens.at[upper_rows], 0)]
    second_copy = load(tokens_hbm.at[lower_rows], tokens.at[lower_rows], 9)
    for i, source in enumerate(order):
        copies.append(load(source, weights.at[i], 1 + i))
    late = [load(shift_hbm, shift, 6), load(extra_hbm, extra, 7)]
    gain_copy = load(gain_hbm, gain_ref, 8)
    smalls = [load(key_gain_hbm, key_gain_ref, 0), load(bias_hbm, bias_ref, 8)]
    rest = [
        load(taps_hbm, taps_ref, 1),
        load(group_gain_hbm, group_gain_ref, 2),
        load(group_shift_hbm, group_shift_ref, 3),
        load(head_gain_hbm, head_gain_ref, 4),
    ]
    copies[0].start()
    second_copy.start()
    gain_copy.start()
    for i, source in enumerate(order):
        for rows in (pl.ds(0, 1024), pl.ds(1024, 1024)):
            load(source.at[rows], weights.at[i, rows], 1 + i).start()
    for copy in late:
        copy.start()

    barrier = pltpu.get_barrier_semaphore()

    def greet(peer):
        pl.semaphore_signal(barrier, inc=1, device_id=peer, device_id_type=MESH)

    greet((sibling, tp))
    pl.when(sp > 0)(lambda: greet((sp - 1, tp)))
    for step in (1, 2, 3):
        meets = (step <= y) | ((z < 3) & (y > 0)) if step == 1 else (step <= y) | (z < 3)
        pl.when(meets)(lambda step=step: greet((y_source(step), tp)))
        pl.when((y == 0) & (step <= z))(
            lambda step=step: greet(((z - step) * 8 + 6 + core, tp))
        )
        pl.when(step <= z)(lambda step=step: greet((sp - 8 * step, tp)))
        greet(x_peer(step))
    targets = (
        4 + jnp.where(sp < 31, 1, 0) + jnp.where(z < 3, jnp.where(y == 3, 2, 3), 3 - y) + (3 - z)
        + jnp.where(y == 3, 3 - z, 0)
    )

    loads = [
        load(gate_hbm, gate_w, 0),
        load(conv_value_hbm, weights.at[5, :, pl.ds(0, PAIR)], 8),
        load(conv_gate_hbm, weights.at[5, :, pl.ds(PAIR, PAIR)], 5),
        load(conv_out_hbm, conv_out_w, 6),
        load(mix_out_hbm, mix_out_w, 7),
    ]
    eye = (iota((HEAD, 2 * PAIR), 0) == iota((HEAD, 2 * PAIR), 1) % HEAD) & (
        iota((HEAD, 2 * PAIR), 1) < PAIR
    )
    identity = jnp.where(eye, 1.0, 0.0).astype(BF16)
    for k in range(3):
        y_seen[k] = identity
        raw_seen[k] = identity
        z_seen[k, 0] = identity[:, :PAIR]
        z_seen[k, 1] = identity[:, PAIR:]
    with jax.named_scope("wait_tokens"):
        copies[0].wait()
        gain_copy.wait()
        for copy in smalls:
            copy.start()
    with jax.named_scope("norm"):
        normed[:128, :] = normalize(tokens[:128, :], gain_ref[...])
        second_copy.wait()
        normed[128:, :] = normalize(tokens[128:, :], gain_ref[...])
    with jax.named_scope("project"):
        found = []
        for i in (0, 2):
            copies[1 + i].wait()
            copies[2 + i].wait()
            found.append(dot(normed[...], weights[i]))
            found.append(dot(normed[...], weights[i + 1]))
        copies[5].wait()
        half = weights.shape[1] // 2
        keep = jnp.where(sp < 32, 1.0, 0.0)
        found.append(
            dot(normed[:, :half], weights[4, :half, :])
            + keep * dot(normed[:, half:], weights[4, half:, :])
        )
        decay, key, rate, receptance, value = (rounded(rows) for rows in found)
        for copy in late + smalls:
            copy.wait()
    for copy in loads[:3] + rest + loads[3:]:
        copy.start()
    with jax.named_scope("algebra"):
        units = chunk_algebra(
            receptance, key, value, decay, rate, key_gain_ref[...], bias_ref[...], shift[...],
            extra[...],
        )
    with jax.named_scope("totals"):
        prefixes = []
        for p in range(2):
            steps = [(u["trans"], u["base"]) for u in units if u["p"] == p]
            two = compose(steps[1], steps[0], dot3)
            upper = compose(steps[3], steps[2], dot3)
            totals[p] = beside(*compose(upper, two, dot3))
            prefixes.append((steps[0], two, steps[2]))
    with jax.named_scope("barrier"):
        pl.semaphore_wait(barrier, targets)
    pair_copy = remote(
        totals.at[1 - core], peer_total, pair_send.at[0], pair_recv.at[0], (sibling, tp)
    )
    pair_copy.start()

    with jax.named_scope("conv_project"):
        for copy in loads[:3]:
            copy.wait()
        gate_rows = dot(normed[...], gate_w[...])
        conv_both = rounded(dot(normed[...], weights[5]))
        conv_input = (conv_both[:, :PAIR] * sigmoid(conv_both[:, PAIR:])).astype(BF16)
        conv_rows[...] = conv_input[224:]
        halo_copy = remote(conv_rows, halo, halo_send.at[0], halo_recv.at[0], (after, tp))
        pl.when(sp < 31)(halo_copy.start)
        extended[:32, :] = jnp.zeros((32, PAIR), F32)
        extended[32:, :] = conv_input.astype(F32)

    with jax.named_scope("gate_project"):
        for copy in rest:
            copy.wait()
        gated = sigmoid(rounded(gate_rows)) * head_gain_ref[...]
        gate_gain[0] = gated[:, :PAIR]
        gate_gain[1] = gated[:, PAIR:]
    with jax.named_scope("pair_wait"):
        pair_copy.wait()
    with jax.named_scope("pair_compose"):
        own, other = totals[core], peer_total[...]
        first = jnp.where(is_first, own, other)
        second = jnp.where(is_first, other, own)
        chip_first = (first[:, :PAIR], first[:, PAIR:])
        chip = compose((second[:, :PAIR], second[:, PAIR:]), chip_first, dot3)
        y_slots[y] = beside(*chip).astype(BF16)

    def y_copy(step, slot, peer):
        return remote(
            y_slots.at[slot], y_slots.at[slot], y_send.at[step - 1], y_recv.at[step - 1],
            (peer, tp),
        )

    def raw_copy(up, slot, plane, peer):
        return remote(
            y_slots.at[slot], raw_slots.at[plane], raw_send.at[up - 1], raw_recv.at[plane],
            (peer, tp),
        )

    def raw_target(up):
        return (z + up) * 8 + core

    for up in (1, 2, 3):
        pl.when((y == 3) & (z + up < 4))(
            lambda up=up: raw_copy(up, y, z, raw_target(up)).start()
        )

    def y_sends(step):
        return (y + step < 4) | ((z < 3) & (y < 3)) if step == 1 else (y + step < 4) | (z < 3)

    for step in (2, 3, 1):
        pl.when(y_sends(step))(lambda step=step: y_copy(step, y, y_target(step)).start())

    with jax.named_scope("local_reads"):
        local_reads(units)
        for p in range(2):
            one, two, third = prefixes[p]
            earlier = (None, one, two, compose(third, two, dot1))
            for u in units:
                if u["p"] != p:
                    continue
                c = u["c"]
                rows = slice(c * CHUNK, (c + 1) * CHUNK)
                if c == 0:
                    local_rows[p, rows] = u["local"]
                    carried_rows[p, rows] = u["carried"]
                    continue
                right = beside(diagonal(earlier[c][0]), diagonal(earlier[c][1]))
                out = dot1(u["carried"], right)
                carried_rows[p, rows] = out[:, :PAIR]
                local_rows[p, rows] = out[:, PAIR:] + u["local"]

    with jax.named_scope("y_wait_lower"):
        for step in (1, 2, 3):

            @pl.when(step <= y)
            def _(step=step):
                y_copy(step, y - step, sibling).wait_recv()
                y_seen[y - step] = y_slots[y - step]

    def slot(ref, k):
        both = ref[k].astype(F32)
        return both[:, :PAIR], both[:, PAIR:]

    with jax.named_scope("before_chip"):
        before_chip = compose(
            slot(y_seen, 2), compose(slot(y_seen, 1), slot(y_seen, 0), dot1), dot3
        )
        before_second = compose(chip_first, before_chip, dot3)
        trans_both = jnp.concatenate([before_chip[0], before_second[0]], axis=0)
        base_both = jnp.concatenate([before_chip[1], before_second[1]], axis=0)

    def z_copy(up, slot, peer, whole):
        part = z_slots.at[slot] if whole else z_slots.at[slot, 1]
        return remote(part, part, z_send.at[up - 1], z_recv.at[slot], (peer, tp))

    def z_column(up):
        pl.when(z > 0)(lambda: z_copy(up, z, sp + 8 * up, True).start())
        pl.when(z == 0)(lambda: z_copy(up, z, sp + 8 * up, False).start())

    def upper(step):
        y_copy(step, lax.rem(y + 4 - step, 4), sibling).wait_recv()

    with jax.named_scope("plane"):

        @pl.when(z < 3)
        def _():
            pl.when(y < 3)(lambda: upper(3))
            lower = compose(slot(y_slots, 1), slot(y_slots, 0), dot1)
            pl.when(y < 2)(lambda: upper(2))

            def store(total):
                z_slots[z, 0] = total[0].astype(BF16)
                z_slots[z, 1] = total[1].astype(BF16)

            @pl.when(y == 0)
            def _():
                store(compose(slot(y_slots, 2), lower, dot3))

            @pl.when(y > 0)
            def _():
                store(compose(compose(slot(y_slots, 3), slot(y_slots, 2), dot1), lower, dot3))

            z_column(1)
            pl.when(z < 2)(lambda: z_column(2))
            pl.when(z < 1)(lambda: z_column(3))

    with jax.named_scope("halo_wait"):

        @pl.when(sp > 0)
        def _():
            halo_copy.wait_recv()
            extended[:32, :] = halo[...].astype(F32)

    with jax.named_scope("convolution"):
        taps = taps_ref[...]
        conv_sum = jnp.zeros((256, PAIR), F32)
        for j in range(31):
            conv_sum = conv_sum + taps[j : j + 1] * extended[pl.ds(2 + j, 256), :]
        normal = group_norm(conv_sum, group_ones(PAIR), GROUP_EPS)
        affine = normal * group_gain_ref[...] + group_shift_ref[...]
        conv_out = (affine * sigmoid(affine)).astype(BF16)
        for k in range(4):
            conv_full[0, k] = conv_out[k * 64 : (k + 1) * 64]
    for step in (2, 1, 3):
        copy = remote(
            conv_full.at[0, x_of(step)], conv_full.at[1, tp],
            conv_send.at[0], conv_recv.at[0], x_peer(step),
        )
        copy.start()

    def z_arrival(below):
        pl.when(below > 0)(lambda: z_copy(1, below, sibling, True).wait_recv())
        pl.when(below == 0)(lambda: z_copy(1, below, sibling, False).wait_recv())

    with jax.named_scope("z_wait"):
        for below in range(2):

            @pl.when(below < z - 1)
            def _(below=below):
                z_arrival(below)
                if below > 0:
                    z_seen[below, 0] = z_slots[below, 0]
                z_seen[below, 1] = z_slots[below, 1]

        for below in range(3):

            @pl.when((y == 0) & (below < z))
            def _(below=below):
                raw_copy(1, 0, below, sibling).wait_recv()
                raw_seen[jnp.where(below < z - 1, below, 2)] = raw_slots[below]

        def through(parts, state):
            return dot3(parts[0], diagonal(state)) + parts[1]

        def plane_below(k):
            return z_seen[k, 0].astype(F32), z_seen[k, 1].astype(F32)

        far = through(slot(raw_seen, 0), z_seen[0, 1].astype(F32))
        far = through(slot(raw_seen, 1), through(plane_below(1), far))
        passed = raw_seen[2]
        out = dot3(
            trans_both,
            beside(
                diagonal(passed[:, :PAIR].astype(F32)), diagonal(passed[:, PAIR:].astype(F32))
            ),
        )
        trans_last, base_last = out[:, :PAIR], out[:, PAIR:] + base_both

        @pl.when(z > 0)
        def _():
            z_arrival(z - 1)

            @pl.when(z > 1)
            def _():
                z_seen[2, 0] = z_slots[z - 1, 0]

            z_seen[2, 1] = z_slots[z - 1, 1]

    with jax.named_scope("z_compose"):
        entering = through(plane_below(2), far)
        states = dot3(trans_last, diagonal(entering)) + base_last
        state_first, state_second = states[:HEAD], states[HEAD:]
        mine = jnp.where(is_first, state_first, state_second)
        pair_states[0] = jnp.where(is_first, state_second, state_first)
    state_copy = remote(
        pair_states.at[0], pair_states.at[1], pair_send.at[0], pair_recv.at[1], (sibling, tp)
    )
    state_copy.start()

    ones = group_ones(PAIR)

    def read_pair(p, state, half):
        readout = local_rows[p] + dot3(carried_rows[p], diagonal(state))
        scale = lax.rsqrt(dot2(readout * readout, ones) * (1.0 / HEAD) + HEAD_EPS)
        mix_out = (readout * scale * gate_gain[p]).astype(BF16)
        for k in range(4):
            mix_sent[half, k] = mix_out[k * 64 : (k + 1) * 64]
        for step in (2, 1, 3):
            copy = remote(
                mix_sent.at[half, x_of(step)], mix_full.at[half, tp],
                mix_send.at[half], mix_recv.at[half, step - 1], x_peer(step),
            )
            copy.start()

    def out_rows(owner, p):
        return pl.ds(pl.multiple_of(owner * 256 + p * PAIR, PAIR), PAIR)

    with jax.named_scope("read_own"):
        read_pair(core, mine, 0)

    with jax.named_scope("own_out"):
        loads[3].wait()
        loads[4].wait()
        acc[...] = dot(
            conv_full[0, tp], conv_out_w[pl.ds(pl.multiple_of(tp * PAIR, PAIR), PAIR), :]
        ) + dot(mix_sent[0, tp], mix_out_w[out_rows(tp, core), :])
    with jax.named_scope("state_wait"):
        state_copy.wait()
    with jax.named_scope("read_other"):
        read_pair(1 - core, pair_states[1], 1)
    conv_all = remote(
        conv_full.at[0, pl.ds(0, 3)], conv_full.at[1, pl.ds(0, 3)], conv_send.at[0],
        conv_recv.at[0], x_peer(1),
    )
    with jax.named_scope("conv_out"):
        conv_all.wait_recv()
        for step in (1, 3, 2):
            arrived = x_of(4 - step)
            rows = pl.ds(pl.multiple_of(arrived * PAIR, PAIR), PAIR)
            acc[...] += dot(conv_full[1, arrived], conv_out_w[rows, :])
    with jax.named_scope("mix_own"):
        acc[...] += dot(mix_sent[1, tp], mix_out_w[out_rows(tp, 1 - core), :])
    conv_all.wait_send()
    pl.when(sp < 31)(halo_copy.wait_send)
    for step in (1, 2, 3):
        pl.when(y_sends(step))(lambda step=step: y_copy(step, y, y_target(step)).wait_send())

        @pl.when(z + step < 4)
        def _(step=step):
            pl.when(z > 0)(lambda: z_copy(step, z, sp + 8 * step, True).wait_send())
            pl.when(z == 0)(lambda: z_copy(step, z, sp + 8 * step, False).wait_send())

        pl.when((y == 3) & (z + step < 4))(
            lambda step=step: raw_copy(step, y, z, raw_target(step)).wait_send()
        )

    for half in (0, 1):
        for step in (1, 3, 2):
            arrived = x_of(4 - step)
            with jax.named_scope("mix_wait"):
                remote(
                    mix_sent.at[half, arrived], mix_full.at[half, arrived],
                    mix_send.at[half], mix_recv.at[half, step - 1], x_peer(step),
                ).wait_recv()
            with jax.named_scope("mix_project"):
                p = core if half == 0 else 1 - core
                acc[...] += dot(mix_full[half, arrived], mix_out_w[out_rows(arrived, p), :])
    with jax.named_scope("final"):
        out_ref[...] = acc[...].astype(BF16)
    for half in (0, 1):
        block = mix_sent.at[half, pl.ds(0, 3)]
        remote(block, block, mix_send.at[half], mix_recv.at[half, 0], x_peer(1)).wait_send()


VMEM = pl.BlockSpec(memory_space=pltpu.VMEM)
ANY = pl.BlockSpec(memory_space=pltpu.HBM)


def local(
    tokens, input_norm_gain, convolution_value_weight, convolution_gate_weight,
    depthwise_taps_weight, convolution_group_gain, convolution_group_shift, receptance_weight,
    key_weight, value_weight, decay_weight, correction_rate_weight, output_gate_weight,
    key_prenorm_gain, decay_offset_bias, position_decay_shift, extra_log_decay, head_norm_gain,
    convolution_output_weight, attention_output_weight,
):
    dma = pltpu.SemaphoreType.DMA
    return pl.pallas_call(
        layer_kernel,
        name="layer",
        out_shape=pltpu.VMEM((64, 2048), BF16),
        in_specs=[ANY] * 20,
        out_specs=VMEM,
        scratch_shapes=[
            pltpu.VMEM((1, 2048), F32),
            pltpu.VMEM((1, 256), F32),
            pltpu.VMEM((1, 256), F32),
            pltpu.VMEM((31, 128), F32),
            pltpu.VMEM((1, 128), F32),
            pltpu.VMEM((1, 128), F32),
            pltpu.VMEM((1, 256), F32),
            pltpu.VMEM((256, 2048), BF16),
            pltpu.VMEM((256, 2048), BF16),
            pltpu.VMEM((6, 2048, 256), BF16),
            pltpu.VMEM((256, 256), F32),
            pltpu.VMEM((256, 256), F32),
            pltpu.VMEM((2048, 256), BF16),
            pltpu.VMEM((512, 2048), BF16),
            pltpu.VMEM((1024, 2048), BF16),
            pltpu.VMEM((2, 64, 256), F32),
            pltpu.VMEM((64, 256), F32),
            pltpu.VMEM((2, 64, 128), F32),
            pltpu.VMEM((4, 64, 256), BF16),
            pltpu.VMEM((4, 2, 64, 128), BF16),
            pltpu.VMEM((3, 64, 256), BF16),
            pltpu.VMEM((3, 2, 64, 128), BF16),
            pltpu.VMEM((3, 64, 256), BF16),
            pltpu.VMEM((3, 64, 256), BF16),
            pltpu.VMEM((288, 128), F32),
            pltpu.VMEM((32, 128), BF16),
            pltpu.VMEM((32, 128), BF16),
            pltpu.VMEM((2, 256, 128), F32),
            pltpu.VMEM((2, 256, 128), F32),
            pltpu.VMEM((2, 256, 128), F32),
            pltpu.VMEM((2, 4, 64, 128), BF16),
            pltpu.VMEM((2, 4, 64, 128), BF16),
            pltpu.VMEM((2, 4, 64, 128), BF16),
            pltpu.VMEM((64, 2048), F32),
            dma((10,)), dma((1,)), dma((2,)), dma((3,)), dma((3,)), dma((3,)), dma((3,)),
            dma((1,)), dma((1,)), dma((1,)), dma((1,)), dma((2,)), dma((2, 3)), dma((3,)), dma((3,)),
        ],
        compiler_params=pltpu.CompilerParams(
            collective_id=0, has_side_effects=True, vmem_limit_bytes=56000000
        ),
    )(
        *(
            pltpu.with_memory_space_constraint(operand, pltpu.HBM)
            for operand in (
                tokens, input_norm_gain.reshape(1, -1), decay_weight, key_weight,
                correction_rate_weight, receptance_weight, value_weight,
                key_prenorm_gain.reshape(1, -1), decay_offset_bias.reshape(1, -1),
                position_decay_shift, extra_log_decay, convolution_value_weight,
                convolution_gate_weight, output_gate_weight, depthwise_taps_weight,
                convolution_group_gain.reshape(1, -1), convolution_group_shift.reshape(1, -1),
                head_norm_gain.reshape(1, -1), convolution_output_weight, attention_output_weight,
            )
        )
    )


def solution(mesh):
    rows, chans, vec = P("sp", None), P(None, "tp"), P("tp")
    placed = (
        rows, P(), chans, chans, chans, vec, vec, chans, chans, chans, chans, chans, chans,
        vec, vec, P("sp", "tp"), P("sp", "tp"), vec, P(), P(),
    )
    return jax.shard_map(
        local, mesh=mesh, in_specs=placed, out_specs=P(("sp", "tp"), None), check_vma=False
    )
```
